128 devices in a mesh: kv: 16 (over z, x), tp: 8 (over y, core).
Axes of the slice: x: 4, y: 4, z: 4, core: 2. Of those that a mesh axis runs over, the one named last changes fastest.
Arguments:
- tokens: bfloat16 [32768, 2048], P('kv'), may hold values from -6 to 6
- norm_gain: bfloat16 [2048], replicated, may hold values from 0.099609375 to 1.8984375
- query_weight: bfloat16 [2048, 1024], P(None, 'tp'), may hold values from -0.125 to 0.125
- cmp_key_weight: bfloat16 [2048, 512], P(None, 'tp'), may hold values from -0.125 to 0.125
- cmp_value_weight: bfloat16 [2048, 512], P(None, 'tp'), may hold values from -0.125 to 0.125
- sel_key_weight: bfloat16 [2048, 512], P(None, 'tp'), may hold values from -0.125 to 0.125
- sel_value_weight: bfloat16 [2048, 512], P(None, 'tp'), may hold values from -0.125 to 0.125
- branch_weight: bfloat16 [2, 2048, 16], replicated, may hold values from -0.125 to 0.125
- key_embed: bfloat16 [8, 32, 64], P('tp'), may hold values from -3 to 3
- key_inner: bfloat16 [8, 2048, 64], P('tp'), may hold values from -0.125 to 0.125
- key_outer: bfloat16 [8, 64, 64], P('tp'), may hold values from -0.75 to 0.75
- value_embed: bfloat16 [8, 32, 64], P('tp'), may hold values from -3 to 3
- value_inner: bfloat16 [8, 2048, 64], P('tp'), may hold values from -0.125 to 0.125
- value_outer: bfloat16 [8, 64, 64], P('tp'), may hold values from -0.75 to 0.75
- out_weight: bfloat16 [1024, 2048], replicated, may hold values from -0.1875 to 0.1875
- chosen: int32 [8, 256, 8], P('tp'), may hold values from 0 to 511, as said below
Outputs:
- attended: bfloat16 [32768, 2048], P(('kv', 'tp'))
The draws below stay inside these ranges and needn't reach their ends.
Inputs may be any that keep to these rules, and one draw needn't show every extreme that they name: `chosen`: each entry is the index of a block of 64 positions in the whole sequence. For every key head and query block, its 8 entries lie in 8 different aligned spans of 2048 positions (at most one from any span), and none lies inside the query block's own positions.
All inputs are finite; a program needn't handle non-finite values.
Results may differ from the reference program's by a relative error of at most 0.0075.
Values may be sent and summed in bfloat16 or wider, within the bound.
A program may use at most 128 MiB of HBM per device.

```python
import jax
import jax.numpy as jnp
from jax import lax

D = 2048
HEADS = 16
KV_HEADS = 8
HEAD_DIM = 64
CMP_BLOCK = 32
SEL_BLOCK = 64
Q_BLOCK = 128
FAR_PICKS = 8
TOK_DEV = 2048
SEQ = 32768


def draw_chosen(key, part):
    interval_limits = SEQ // TOK_DEV
    per_span = TOK_DEV // Q_BLOCK
    span_blocks = TOK_DEV // SEL_BLOCK
    own_blocks = Q_BLOCK // SEL_BLOCK
    query_blocks = SEQ // Q_BLOCK
    key_noise, key_inner, key_shift = jax.random.split(key, 3)
    diagonal_group = jnp.arange(query_blocks, dtype=jnp.int32) // per_span
    local_index = jnp.arange(query_blocks, dtype=jnp.int32) % per_span
    eligible_group = jnp.arange(interval_limits, dtype=jnp.int32)
    jitter_perturbation = jax.random.randint(key_noise, (KV_HEADS, query_blocks, interval_limits), 0, 2 ** 16)
    preference_increment = jnp.where(eligible_group[None, :] <= diagonal_group[:, None], 2 ** 24, 0)
    preference_increment = preference_increment + jnp.where(eligible_group[None, :] == diagonal_group[:, None] - 1, 2 ** 26, 0)
    preference_increment = preference_increment + jnp.where(eligible_group[None, :] == diagonal_group[:, None] - interval_limits // 2, 2 ** 26, 0)
    preference_increment = preference_increment + jnp.where(eligible_group[None, :] == 0, 2 ** 25, 0)
    group_relevance = jitter_perturbation * interval_limits + eligible_group[None, None, :] + preference_increment[None]
    _, picked = lax.top_k(group_relevance, FAR_PICKS)
    inside = jax.random.randint(key_inner, (KV_HEADS, query_blocks, FAR_PICKS), 0, span_blocks)
    offset = jax.random.randint(key_shift, (KV_HEADS, query_blocks, FAR_PICKS), 0, span_blocks - own_blocks)
    shifted = (local_index[None, :, None] * own_blocks + own_blocks + offset) % span_blocks
    within = jnp.where(picked == diagonal_group[None, :, None], shifted, inside)
    return (picked * span_blocks + within).astype(jnp.int32)


def block_scale(rng, dims, pieces, smallest, top_value):
    def one(axis_at, blocks):
        draws = jax.random.uniform(jax.random.fold_in(jax.random.fold_in(rng, 6), axis_at), (blocks,), jnp.float32, smallest / len(pieces), top_value / len(pieces))
        return jnp.repeat(jnp.exp(draws), dims[axis_at] // blocks).reshape((-1,) + (1,) * (len(dims) - axis_at - 1))

    factor_of = one(*pieces[0])
    for cut in pieces[1:]:
        factor_of = factor_of * one(*cut)
    return factor_of


def bell_draw(own_key, shape, scale, bound, cuts=(), kind=jnp.bfloat16):
    level = block_scale(own_key, shape, cuts, -0.22, 0.18) if cuts else 1.0
    result = jax.random.normal(own_key, shape, jnp.float32) * scale * level
    return jnp.minimum(jnp.maximum(result, -bound), bound).astype(kind)


def setup_inputs(seed: int = 0) -> dict:
    splits = jax.random.split(jax.random.key(seed), 17)
    return {
        "tokens": bell_draw(splits[0], (SEQ, D), 1.0, 6.0, ((0, 16),)),
        "norm_gain": jnp.clip(1.0 + 0.18 * jax.random.normal(splits[1], (D,), jnp.float32), 0.099609375, 1.8984375).astype(jnp.bfloat16),
        "query_weight": bell_draw(splits[2], (D, HEADS * HEAD_DIM), D ** -0.5, 0.125, ((1, 8),)),
        "cmp_key_weight": bell_draw(splits[3], (D, KV_HEADS * HEAD_DIM), D ** -0.5, 0.125, ((1, 8),)),
        "cmp_value_weight": bell_draw(splits[4], (D, KV_HEADS * HEAD_DIM), D ** -0.5, 0.125, ((1, 8),)),
        "sel_key_weight": bell_draw(splits[5], (D, KV_HEADS * HEAD_DIM), D ** -0.5, 0.125, ((1, 8),)),
        "sel_value_weight": bell_draw(splits[6], (D, KV_HEADS * HEAD_DIM), D ** -0.5, 0.125, ((1, 8),)),
        "branch_weight": bell_draw(splits[7], (2, D, HEADS), D ** -0.5, 0.125),
        "key_embed": bell_draw(splits[8], (KV_HEADS, CMP_BLOCK, HEAD_DIM), 0.5, 3.0, ((0, 8),)),
        "key_inner": bell_draw(splits[9], (KV_HEADS, CMP_BLOCK * HEAD_DIM, HEAD_DIM), (CMP_BLOCK * HEAD_DIM) ** -0.5, 0.125, ((0, 8),)),
        "key_outer": bell_draw(splits[10], (KV_HEADS, HEAD_DIM, HEAD_DIM), HEAD_DIM ** -0.5, 0.75, ((0, 8),)),
        "value_embed": bell_draw(splits[11], (KV_HEADS, CMP_BLOCK, HEAD_DIM), 0.5, 3.0, ((0, 8),)),
        "value_inner": bell_draw(splits[12], (KV_HEADS, CMP_BLOCK * HEAD_DIM, HEAD_DIM), (CMP_BLOCK * HEAD_DIM) ** -0.5, 0.125, ((0, 8),)),
        "value_outer": bell_draw(splits[13], (KV_HEADS, HEAD_DIM, HEAD_DIM), HEAD_DIM ** -0.5, 0.75, ((0, 8),)),
        "out_weight": bell_draw(splits[14], (HEADS * HEAD_DIM, D), (HEADS * HEAD_DIM) ** -0.5, 0.1875),
        "chosen": draw_chosen(jax.random.fold_in(splits[16], 71), 0),
    }


ROPE_BASE = 10000.0
norm_eps = 1e-06
masked_score = -1000000000.0

def rotate(values_in, positions):
    half_dim = values_in.shape[-1] // 2
    inverse = ROPE_BASE ** (-jnp.arange(half_dim, dtype=jnp.float32) / half_dim)
    rotary_phases = positions.astype(jnp.float32)[:, None] * inverse[None, :]
    cosine = jnp.cos(rotary_phases)[:, None, :]
    sine = jnp.sin(rotary_phases)[:, None, :]
    first_half = values_in[..., :half_dim]
    second_half = values_in[..., half_dim:]
    return jnp.concatenate([first_half * cosine - second_half * sine, second_half * cosine + first_half * sine], axis=-1)

def summarize(raw_rows, embed, inner, outer):
    block_count = raw_rows.shape[0] // CMP_BLOCK
    blocked = raw_rows.reshape(block_count, CMP_BLOCK, KV_HEADS, HEAD_DIM).transpose(2, 0, 1, 3).astype(jnp.float32)
    blocked = (blocked + embed.astype(jnp.float32)[:, None]).astype(jnp.bfloat16)
    blocked = blocked.reshape(KV_HEADS, block_count, CMP_BLOCK * HEAD_DIM)
    hidden = jax.nn.gelu(jnp.einsum('knc,kce->kne', blocked.astype(jnp.float32), inner.astype(jnp.float32))).astype(jnp.bfloat16)
    return jnp.einsum('kne,kef->knf', hidden.astype(jnp.float32), outer.astype(jnp.float32)).astype(jnp.bfloat16)

def reference(tokens, norm_gain, query_weight, cmp_key_weight, cmp_value_weight, sel_key_weight, sel_value_weight, branch_weight, key_embed, key_inner, key_outer, value_embed, value_inner, value_outer, out_weight, chosen):
    length = tokens.shape[0]
    group_size = HEADS // KV_HEADS
    positions = jnp.arange(length, dtype=jnp.int32)
    scale = HEAD_DIM ** (-0.5)
    expanded_mask = tokens.astype(jnp.float32)
    normed = (expanded_mask * lax.rsqrt(lax.optimization_barrier(jnp.mean(expanded_mask * expanded_mask, axis=-1, keepdims=True)) + norm_eps) * norm_gain.astype(jnp.float32)).astype(jnp.bfloat16)

    def project(weight_in):
        return jnp.dot(normed, weight_in, preferred_element_type=jnp.float32)
    query = project(query_weight).reshape(length, HEADS, HEAD_DIM)
    q_plain = query.astype(jnp.bfloat16)
    q_turn = rotate(query, positions).astype(jnp.bfloat16)
    cmp_key = project(cmp_key_weight).astype(jnp.bfloat16).reshape(length, KV_HEADS, HEAD_DIM)
    cmp_value = project(cmp_value_weight).astype(jnp.bfloat16).reshape(length, KV_HEADS, HEAD_DIM)
    sel_key = rotate(project(sel_key_weight).reshape(length, KV_HEADS, HEAD_DIM), positions).astype(jnp.bfloat16)
    selected_value = project(sel_value_weight).astype(jnp.bfloat16).reshape(length, KV_HEADS, HEAD_DIM)
    gate_cmp = jax.nn.sigmoid(project(branch_weight[0]))
    gate_sel = jax.nn.sigmoid(project(branch_weight[1]))
    summary_key = summarize(cmp_key, key_embed, key_inner, key_outer)
    summary_value = summarize(cmp_value, value_embed, value_inner, value_outer)
    summary_count = summary_key.shape[1]
    block_end = (jnp.arange(summary_count, dtype=jnp.int32) + 1) * CMP_BLOCK - 1

    def compress_head(packed_rows):
        head_query, head_keys, head_values = packed_rows
        scores = jnp.einsum('tgd,cd->tgc', head_query.astype(jnp.float32), head_keys.astype(jnp.float32)) * scale
        allowed_keys = (block_end[None, :] <= positions[:, None])[:, None, :]
        probs = jax.nn.softmax(jnp.where(allowed_keys, scores, masked_score), axis=-1) * allowed_keys.astype(jnp.float32)
        return jnp.einsum('tgc,cd->tgd', probs.astype(jnp.bfloat16).astype(jnp.float32), head_values.astype(jnp.float32))
    q_group = q_plain.reshape(length, KV_HEADS, group_size, HEAD_DIM).transpose(1, 0, 2, 3)
    out_cmp = lax.map(compress_head, (q_group, summary_key, summary_value))
    out_cmp = out_cmp.transpose(1, 0, 2, 3).reshape(length, HEADS, HEAD_DIM)
    query_blocks = length // Q_BLOCK
    block_pos = jnp.arange(query_blocks, dtype=jnp.int32)[:, None] * Q_BLOCK + jnp.arange(Q_BLOCK, dtype=jnp.int32)[None, :]

    def select_head(packed_rows):
        head_query, head_keys, head_values, head_picks = packed_rows
        far_keys = head_keys.reshape(-1, SEL_BLOCK, HEAD_DIM)[head_picks].reshape(query_blocks, FAR_PICKS * SEL_BLOCK, HEAD_DIM)
        far_values = head_values.reshape(-1, SEL_BLOCK, HEAD_DIM)[head_picks].reshape(query_blocks, FAR_PICKS * SEL_BLOCK, HEAD_DIM)
        all_keys = jnp.concatenate([head_keys.reshape(query_blocks, Q_BLOCK, HEAD_DIM), far_keys], axis=1)
        all_values = jnp.concatenate([head_values.reshape(query_blocks, Q_BLOCK, HEAD_DIM), far_values], axis=1)
        far_pos = (head_picks[:, :, None] * SEL_BLOCK + jnp.arange(SEL_BLOCK, dtype=jnp.int32)[None, None, :]).reshape(query_blocks, -1)
        key_pos = jnp.concatenate([block_pos, far_pos], axis=1)
        allowed_keys = key_pos[:, None, None, :] <= block_pos[:, :, None, None]
        scores = jnp.einsum('nqgd,nmd->nqgm', head_query.astype(jnp.float32), all_keys.astype(jnp.float32)) * scale
        probs = jax.nn.softmax(jnp.where(allowed_keys, scores, masked_score), axis=-1)
        return jnp.einsum('nqgm,nmd->nqgd', probs.astype(jnp.bfloat16).astype(jnp.float32), all_values.astype(jnp.float32))
    q_sel = q_turn.reshape(query_blocks, Q_BLOCK, KV_HEADS, group_size, HEAD_DIM).transpose(2, 0, 1, 3, 4)
    out_sel = lax.map(select_head, (q_sel, sel_key.transpose(1, 0, 2), selected_value.transpose(1, 0, 2), chosen.astype(jnp.int32)))
    out_sel = out_sel.transpose(1, 2, 0, 3, 4).reshape(length, HEADS, HEAD_DIM)
    mixed = (gate_cmp[..., None] * out_cmp + gate_sel[..., None] * out_sel).reshape(length, HEADS * HEAD_DIM).astype(jnp.bfloat16)
    return jnp.dot(mixed, out_weight, preferred_element_type=jnp.float32).astype(jnp.bfloat16)
```

```python
import functools

import jax
import jax.numpy as jnp
import numpy as np
from jax import lax
from jax.experimental import pallas as pl
from jax.experimental.pallas import tpu as pltpu
from jax.sharding import PartitionSpec as P

HEAD_DIM = 64
CMP_BLOCK = 32
SEL_BLOCK = 64
Q_BLOCK = 128
FAR_PICKS = 8
LANES = 2 * HEAD_DIM
PLANES = 4
ACROSS = 4
OWNERS = PLANES * ACROSS
RANKS = 8
MESH = pl.DeviceIdType.MESH

ROPE_BASE = 10000.0
norm_eps = 1e-06
MASKED = -1e30

MOVES = [(dz, dx) for dx in (2, 1, 3, 0) for dz in (2, 1, 3, 0) if (dz, dx) != (0, 0)]
EARLY = 5


def nt_dot(a, b):
    return lax.dot_general(a, b, (((1,), (1,)), ((), ())), preferred_element_type=jnp.float32)


def low_lanes(shape):
    return lax.broadcasted_iota(jnp.int32, shape, 1) < HEAD_DIM


def gate_lanes(gate, first, shape):
    return jnp.where(low_lanes(shape), gate[:, first : first + 1], gate[:, first + 1 : first + 2])


def merge(out, rows):
    low = low_lanes((rows, LANES))
    return jnp.where(low, pltpu.roll(out[:rows], HEAD_DIM, 1), out[rows:])


def layer_kernel(
    chosen_ref,
    gain_ref,
    ke_ref,
    ko_ref,
    ve_ref,
    vo_ref,
    lo_ref,
    hi_hbm,
    tok_hbm,
    wq_hbm,
    wsk_hbm,
    wsv_hbm,
    wck_hbm,
    wcv_hbm,
    wg_hbm,
    ki_hbm,
    vi_hbm,
    wo_hbm,
    out_ref,
    hi,
    tok,
    wq,
    raw,
    wt,
    ki,
    vi,
    wo,
    held,
    stage,
    got,
    qp,
    qt,
    ckv,
    gate,
    scales,
    sums,
    oc,
    mix,
    heard,
    pick_vm,
    pick_sm,
    near_sm,
    tok_sem,
    local_sem,
    send_sem,
    recv_sem,
    sum_send,
    sum_recv,
    mix_send,
    mix_recv,
):
    me, rank = lax.axis_index("kv"), lax.axis_index("tp")
    z, x = me // ACROSS, me % ACROSS
    rows, width = tok.shape
    tile = 512
    tiles = rows // tile
    q_blocks = rows // Q_BLOCK
    span = rows // SEL_BLOCK
    blocks = rows // CMP_BLOCK
    scale = HEAD_DIM ** (-0.5)

    sums[...] = jnp.zeros_like(sums)
    barrier = pltpu.get_barrier_semaphore()
    for d in range(1, OWNERS):
        pl.semaphore_signal(barrier, inc=1, device_id={"kv": (me + d) % OWNERS}, device_id_type=MESH)
    for d in range(1, RANKS):
        pl.semaphore_signal(barrier, inc=1, device_id={"tp": (rank + d) % RANKS}, device_id_type=MESH)

    loads = [
        (wq_hbm, wq),
        (wsk_hbm, raw.at[pl.ds(0, 64)]),
        (wsv_hbm, raw.at[pl.ds(64, 64)]),
        (wck_hbm, raw.at[pl.ds(128, 64)]),
        (wcv_hbm, raw.at[pl.ds(192, 64)]),
        (wg_hbm, raw.at[pl.ds(256, 32)]),
        (hi_hbm.at[pl.ds(pl.multiple_of(me * span, span), span)], hi),
        (ki_hbm, ki),
        (vi_hbm, vi),
        (wo_hbm, wo),
    ]
    copies = [pltpu.make_async_copy(a, b, local_sem.at[n]) for n, (a, b) in enumerate(loads)]
    tok_copies = [
        pltpu.make_async_copy(tok_hbm.at[pl.ds(n * tile, tile)], tok.at[pl.ds(n * tile, tile)], tok_sem.at[n])
        for n in range(tiles)
    ]
    for copy in copies[:7]:
        copy.start()
    for copy in tok_copies:
        copy.start()
    for copy in copies[7:]:
        copy.start()

    chosen = chosen_ref[...]
    mine = jnp.where(chosen // span == me, chosen % span, 0)
    pick_vm[0] = jnp.broadcast_to(jnp.sum(mine, axis=0, keepdims=True), chosen.shape)
    pick_vm[1] = chosen
    to_smem = pltpu.make_async_copy(pick_vm.at[0], pick_sm, local_sem.at[len(loads)])
    near_smem = pltpu.make_async_copy(pick_vm.at[1], near_sm, local_sem.at[len(loads) + 1])
    to_smem.start()
    near_smem.start()

    for copy in copies[:7]:
        copy.wait()

    gain = gain_ref[...].astype(jnp.float32)
    eye = (
        lax.broadcasted_iota(jnp.int32, (LANES, LANES), 0)
        == lax.broadcasted_iota(jnp.int32, (LANES, LANES), 1)
    ).astype(jnp.bfloat16)

    def weigh(source, first, count, target):
        def one(i, carry):
            r = pl.ds(pl.multiple_of(first + i * 16, 16), 16)
            t = pl.ds(pl.multiple_of(target + i * 16, 16), 16)
            wt[t] = (source[r].astype(jnp.float32) * gain).astype(jnp.bfloat16)
            return carry

        lax.fori_loop(0, count // 16, one, 0)

    weigh(raw, 0, 128, 0)
    for c in range(width // 256):
        cut = slice(c * 256, (c + 1) * 256)
        turned = nt_dot(eye, wq[cut])
        wt[128:256, cut] = (turned * gain[:, cut]).astype(jnp.bfloat16)

    first_half = lax.broadcasted_iota(jnp.int32, (1, LANES), 1) % HEAD_DIM < HEAD_DIM // 2
    quarter = HEAD_DIM // 2

    def turn(v, cosine, sine):
        swapped = jnp.where(first_half, pltpu.roll(v, LANES - quarter, 1), pltpu.roll(v, quarter, 1))
        return v * cosine + swapped * sine

    def project(i):
        at = pl.ds(i * tile, tile)
        v = tok[at]
        y = nt_dot(v, wt[0:256])
        w = v.astype(jnp.float32)
        inv = lax.rsqrt(jnp.mean(w * w, axis=-1, keepdims=True) + norm_eps)
        scales[at] = jnp.broadcast_to(inv, (tile, LANES))
        y = y * inv
        cos_lo, sin_lo = lo_ref[0:64], lo_ref[64:128]
        for g in range(tile // SEL_BLOCK):
            b = i * (tile // SEL_BLOCK) + g
            cut = slice(g * SEL_BLOCK, (g + 1) * SEL_BLOCK)
            cos_hi, sin_hi = hi[pl.ds(b, 1), 0:LANES], hi[pl.ds(b, 1), LANES : 2 * LANES]
            cosine = cos_hi * cos_lo - sin_hi * sin_lo
            sine = sin_hi * cos_lo + cos_hi * sin_lo
            sine = jnp.where(first_half, -sine, sine)
            part = y[cut, 0:LANES]
            low = low_lanes(part.shape)
            held[b] = jnp.where(low, turn(part, cosine, sine), part).astype(jnp.bfloat16)
            part = y[cut, LANES : 2 * LANES] * scale
            to = pl.ds(b * SEL_BLOCK, SEL_BLOCK)
            for ref, q in ((qp, part), (qt, turn(part, cosine, sine))):
                ref[0, to] = jnp.where(low, q, 0.0).astype(jnp.bfloat16)
                ref[1, to] = jnp.where(low, pltpu.roll(q, HEAD_DIM, 1), 0.0).astype(jnp.bfloat16)

    for i in range(tiles):
        tok_copies[i].wait()
        project(i)

    to_smem.wait()
    near_smem.wait()
    pl.semaphore_wait(barrier, OWNERS + RANKS - 2)

    def route(dz, dx):
        there = ((z + dz) % PLANES) * ACROSS + (x + dx) % ACROSS
        here = ((z - dz) % PLANES) * ACROSS + (x - dx) % ACROSS
        if dz == 0:
            return there, x + dx < ACROSS, here, x >= dx
        return there, z + dz < PLANES, here, z >= dz

    def block_copy(n, owner):
        there, sends, here, gets = route(*MOVES[n])
        copy = pltpu.make_async_remote_copy(
            src_ref=stage.at[n],
            dst_ref=got.at[owner],
            send_sem=send_sem.at[n],
            recv_sem=recv_sem.at[n],
            device_id={"kv": there},
            device_id_type=MESH,
        )
        return copy, there, sends, gets

    def gather(target, first):
        def one(j, carry):
            target[j] = held[pick_sm[0, first + j]]
            return carry

        lax.fori_loop(0, q_blocks, one, 0)

    def send_blocks(n):
        copy, there, sends, _ = block_copy(n, me)

        def go():
            gather(stage.at[n], there * q_blocks)
            copy.start()

        pl.when(sends)(go)

    for n in range(EARLY):
        send_blocks(n)

    weigh(raw, 128, 160, 256)

    def project_more(i, carry):
        at = pl.ds(pl.multiple_of(i * tile, tile), tile)
        y = nt_dot(tok[at], wt[256:416])
        inv = scales[at]
        ckv[at] = (y[:, 0:LANES] * inv).astype(jnp.bfloat16).astype(jnp.float32)
        gate[at] = jax.nn.sigmoid(y[:, LANES : LANES + 32] * inv[:, 0:32])
        return carry

    lax.fori_loop(0, tiles, project_more, 0)
    for copy in copies[7:9]:
        copy.wait()

    low = low_lanes((blocks, LANES))

    def summarize(is_value, e_ref, i_ref, o_ref):
        parts = []
        for c in range(0, CMP_BLOCK, 2):
            a = ckv[pl.ds(c, blocks, stride=CMP_BLOCK), :]
            b = ckv[pl.ds(c + 1, blocks, stride=CMP_BLOCK), :]
            if is_value:
                pair = jnp.where(low, pltpu.roll(a, HEAD_DIM, 1), b)
            else:
                pair = jnp.where(low, a, pltpu.roll(b, HEAD_DIM, 1))
            e = e_ref[c // 2 : c // 2 + 1, :].astype(jnp.float32)
            parts.append((pair + e).astype(jnp.bfloat16))
        flat = jnp.concatenate(parts, axis=1)
        hidden = jax.nn.gelu(nt_dot(flat, i_ref[...])).astype(jnp.bfloat16)
        return jnp.dot(hidden, o_ref[...], preferred_element_type=jnp.float32)

    sk = summarize(False, ke_ref, ki, ko_ref)
    sv = summarize(True, ve_ref, vi, vo_ref)
    sums[me] = jnp.concatenate([sk, sv], axis=1).astype(jnp.bfloat16)

    def sum_copy(n, owner):
        there, sends, here, gets = route(*MOVES[n])
        copy = pltpu.make_async_remote_copy(
            src_ref=sums.at[owner],
            dst_ref=sums.at[owner],
            send_sem=sum_send.at[n],
            recv_sem=sum_recv.at[n],
            device_id={"kv": there},
            device_id_type=MESH,
        )
        return copy, here, sends, gets

    for n in range(len(MOVES)):
        copy, _, sends, _ = sum_copy(n, me)
        pl.when(sends)(copy.start)
    for n in range(EARLY, len(MOVES)):
        send_blocks(n)
    gather(got.at[me], me * q_blocks)
    for n in range(len(MOVES)):
        _, here, _, gets = sum_copy(n, me)
        copy, _, _, _ = sum_copy(n, here)
        pl.when(gets)(copy.wait_recv)

    part = 256

    def compress(i, carry):
        at = pl.ds(pl.multiple_of(i * part, part), part)
        row = lax.broadcasted_iota(jnp.int32, (2 * part, 1), 0)
        pos = me * rows + i * part + jnp.where(row >= part, row - part, row)
        lane = lax.broadcasted_iota(jnp.int32, (1, OWNERS * blocks), 1)
        allowed = (lane + 1) * CMP_BLOCK - 1 <= pos
        keys = jnp.concatenate([sums[s] for s in range(OWNERS)], axis=0)
        q = jnp.concatenate([qp[0, at], qp[1, at]], axis=0)
        s = jnp.where(allowed, nt_dot(q, keys), MASKED)
        top = jnp.max(s, axis=-1, keepdims=True)
        e = jnp.exp(s - top)
        total = jnp.sum(e, axis=-1, keepdims=True)
        o = jnp.dot(e.astype(jnp.bfloat16), keys, preferred_element_type=jnp.float32)
        o = o * jnp.where(pos >= CMP_BLOCK - 1, 1.0 / total, 0.0)
        o = merge(o, part)
        g = pltpu.roll(pltpu_pad(gate[at]), LANES - 2 * rank, 1)
        oc[at] = o * gate_lanes(g, 0, o.shape)
        return carry

    def pltpu_pad(g):
        return jnp.concatenate([g, g, g, g], axis=1)

    lax.fori_loop(0, rows // part, compress, 0)

    rank_rows = rows // RANKS
    group = rank_rows // Q_BLOCK

    def mix_copy(step):
        target = (rank + 1 + step) % RANKS
        at = pl.ds(pl.multiple_of(target * rank_rows, rank_rows), rank_rows)
        return pltpu.make_async_remote_copy(
            src_ref=mix.at[at],
            dst_ref=heard.at[rank],
            send_sem=mix_send.at[step],
            recv_sem=mix_recv.at[step],
            device_id={"tp": target},
            device_id_type=MESH,
        )

    for n in range(len(MOVES)):
        _, _, here, _ = route(*MOVES[n])
        copy, _, _, gets = block_copy(n, here)
        pl.when(gets)(copy.wait_recv)

    def choose(step, carry):
        target = (rank + 1 + step) % RANKS
        for u in range(group):
            j = target * group + u
            at = pl.ds(pl.multiple_of(j * Q_BLOCK, Q_BLOCK), Q_BLOCK)
            own = j * (Q_BLOCK // SEL_BLOCK)
            parts = [held[own + b] for b in range(Q_BLOCK // SEL_BLOCK)]
            first = me * span + own
            biases = []
            for a in range(FAR_PICKS):
                pick = near_sm[a, me * q_blocks + j]
                usable = pick < first
                owner = jnp.where(usable, pick // span, me)
                parts.append(got[owner, j])
                biases.append(jnp.where(usable, 0.0, MASKED))
            keys = jnp.concatenate(parts, axis=0)
            q = jnp.concatenate([qt[0, at], qt[1, at]], axis=0)
            s = nt_dot(q, keys)
            row = lax.broadcasted_iota(jnp.int32, (2 * Q_BLOCK, Q_BLOCK), 0)
            row = jnp.where(row >= Q_BLOCK, row - Q_BLOCK, row)
            lane = lax.broadcasted_iota(jnp.int32, row.shape, 1)
            pieces = [jnp.where(lane > row, MASKED, s[:, :Q_BLOCK])]
            low = lax.broadcasted_iota(jnp.int32, (1, LANES), 1) < SEL_BLOCK
            for a in range(0, FAR_PICKS, 2):
                c = Q_BLOCK + a * SEL_BLOCK
                pieces.append(s[:, c : c + LANES] + jnp.where(low, biases[a], biases[a + 1]))
            s = jnp.concatenate(pieces, axis=1)
            top = jnp.max(s, axis=-1, keepdims=True)
            e = jnp.exp(s - top)
            total = jnp.sum(e, axis=-1, keepdims=True)
            o = jnp.dot(e.astype(jnp.bfloat16), keys, preferred_element_type=jnp.float32)
            o = merge(o * (1.0 / total), Q_BLOCK)
            g = pltpu.roll(pltpu_pad(gate[at]), LANES - 2 * rank, 1)
            mix[at] = (oc[at] + o * gate_lanes(g, 16, o.shape)).astype(jnp.bfloat16)
        pl.when(step > 0)(lambda: mix_copy(step - 1).start())
        return carry

    lax.fori_loop(0, RANKS, choose, 0)

    own_at = pl.ds(pl.multiple_of(rank * rank_rows, rank_rows), rank_rows)
    heard[rank] = mix[own_at]
    for n in range(len(MOVES)):
        copy, _, sends, _ = block_copy(n, me)
        pl.when(sends)(copy.wait_send)
        copy, _, sends, _ = sum_copy(n, me)
        pl.when(sends)(copy.wait_send)
    copies[9].wait()
    for step in range(RANKS - 1):
        mix_copy(step).wait_send()
        mix_copy(step).wait_recv()

    lhs = jnp.concatenate([heard[t] for t in range(RANKS)], axis=1)

    def finish(c, carry):
        at = pl.ds(pl.multiple_of(c * 512, 512), 512)
        out_ref[:, at] = jnp.dot(lhs, wo[:, at], preferred_element_type=jnp.float32).astype(jnp.bfloat16)
        return carry

    lax.fori_loop(0, width // 512, finish, 0)


def rope_tables(length):
    half = HEAD_DIM // 2
    inverse = ROPE_BASE ** (-(np.arange(half, dtype=np.float32)) / np.float32(half))
    inverse = np.tile(inverse.astype(np.float32).astype(np.float64), LANES // half)

    def table(positions):
        angle = positions.astype(np.float64)[:, None] * inverse[None, :]
        return np.cos(angle), np.sin(angle)

    low = np.concatenate(table(np.arange(SEL_BLOCK)), axis=0).astype(np.float32)
    high = np.concatenate(table(np.arange(length // SEL_BLOCK) * SEL_BLOCK), axis=1).astype(np.float32)
    return jnp.asarray(low), jnp.asarray(high)


def per_device(
    tokens,
    norm_gain,
    query_weight,
    cmp_key_weight,
    cmp_value_weight,
    sel_key_weight,
    sel_value_weight,
    branch_weight,
    key_embed,
    key_inner,
    key_outer,
    value_embed,
    value_inner,
    value_outer,
    out_weight,
    chosen,
):
    rows, width = tokens.shape
    f32, bf16 = jnp.float32, jnp.bfloat16
    low, high = rope_tables(rows * OWNERS)
    span = rows // SEL_BLOCK
    q_blocks = rows // Q_BLOCK
    blocks = rows // CMP_BLOCK
    rank_rows = rows // RANKS
    picks = chosen.shape[1]
    operands = (
        chosen[0].T,
        norm_gain.reshape(1, width),
        key_embed.reshape(CMP_BLOCK // 2, LANES),
        key_outer[0],
        value_embed.reshape(CMP_BLOCK // 2, LANES),
        value_outer[0],
        low,
        high,
        tokens,
        query_weight,
        sel_key_weight.T,
        sel_value_weight.T,
        cmp_key_weight.T,
        cmp_value_weight.T,
        branch_weight.transpose(0, 2, 1).reshape(32, width),
        key_inner[0].T,
        value_inner[0].T,
        out_weight,
    )
    vmem = pl.BlockSpec(memory_space=pltpu.VMEM)
    hbm = pl.BlockSpec(memory_space=pl.ANY)
    dma = pltpu.SemaphoreType.DMA
    moves = len(MOVES)
    return pl.pallas_call(
        layer_kernel,
        in_specs=[vmem] * 7 + [hbm] * 11,
        out_specs=vmem,
        out_shape=jax.ShapeDtypeStruct((rank_rows, width), bf16),
        scratch_shapes=[
            pltpu.VMEM((span, 2 * LANES), f32),
            pltpu.VMEM((rows, width), bf16),
            pltpu.VMEM((width, LANES), bf16),
            pltpu.VMEM((288, width), bf16),
            pltpu.VMEM((416, width), bf16),
            pltpu.VMEM((HEAD_DIM, width), bf16),
            pltpu.VMEM((HEAD_DIM, width), bf16),
            pltpu.VMEM(out_weight.shape, bf16),
            pltpu.VMEM((span, SEL_BLOCK, LANES), bf16),
            pltpu.VMEM((moves, q_blocks, SEL_BLOCK, LANES), bf16),
            pltpu.VMEM((OWNERS, q_blocks, SEL_BLOCK, LANES), bf16),
            pltpu.VMEM((2, rows, LANES), bf16),
            pltpu.VMEM((2, rows, LANES), bf16),
            pltpu.VMEM((rows, LANES), f32),
            pltpu.VMEM((rows, 32), f32),
            pltpu.VMEM((rows, LANES), f32),
            pltpu.VMEM((OWNERS, blocks, LANES), bf16),
            pltpu.VMEM((rows, LANES), f32),
            pltpu.VMEM((rows, LANES), bf16),
            pltpu.VMEM((RANKS, rank_rows, LANES), bf16),
            pltpu.VMEM((2, FAR_PICKS, picks), jnp.int32),
            pltpu.SMEM((FAR_PICKS, picks), jnp.int32),
            pltpu.SMEM((FAR_PICKS, picks), jnp.int32),
            dma((rows // 512,)),
            dma((12,)),
            dma((moves,)),
            dma((moves,)),
            dma((moves,)),
            dma((moves,)),
            dma((RANKS,)),
            dma((RANKS,)),
        ],
        compiler_params=pltpu.CompilerParams(
            collective_id=0, has_side_effects=True, vmem_limit_bytes=60 * 1024 * 1024
        ),
        cost_estimate=pl.CostEstimate(flops=int(4e10), bytes_accessed=int(2e7), transcendentals=0),
        name="layer",
    )(*operands)


def solution(mesh):
    placed = (
        P("kv", None),
        P(),
        P(None, "tp"),
        P(None, "tp"),
        P(None, "tp"),
        P(None, "tp"),
        P(None, "tp"),
        P(),
        P("tp", None, None),
        P("tp", None, None),
        P("tp", None, None),
        P("tp", None, None),
        P("tp", None, None),
        P("tp", None, None),
        P(),
        P("tp", None, None),
    )
    return jax.shard_map(
        per_device, mesh=mesh, in_specs=placed, out_specs=P(("kv", "tp"), None), check_vma=False
    )
```

```python
import functools

import jax
import jax.numpy as jnp
import numpy as np
from jax import lax
from jax.experimental import pallas as pl
from jax.experimental.pallas import tpu as pltpu
from jax.sharding import PartitionSpec as P

HEAD_DIM = 64
CMP_BLOCK = 32
SEL_BLOCK = 64
Q_BLOCK = 128
FAR_PICKS = 8
LANES = 2 * HEAD_DIM
PLANES = 4
ACROSS = 4
OWNERS = PLANES * ACROSS
RANKS = 8
MESH = pl.DeviceIdType.MESH

ROPE_BASE = 10000.0
norm_eps = 1e-06
MASKED = -1e30

MOVES = [(dz, dx) for dx in (2, 1, 3, 0) for dz in (2, 1, 3, 0) if (dz, dx) != (0, 0)]
OWN, NEAR, FAR, SKIP = range(4)
HOPS = [(kind, dx) for kind in (OWN, NEAR, FAR) for dx in (2, 1, 3)] + [(SKIP, dx) for dx in (2, 1, 3, 0)]


def nt_dot(a, b):
    return lax.dot_general(a, b, (((1,), (1,)), ((), ())), preferred_element_type=jnp.float32)


def low_lanes(shape):
    return lax.broadcasted_iota(jnp.int32, shape, 1) < HEAD_DIM


def gate_lanes(gate, first, shape):
    return jnp.where(low_lanes(shape), gate[:, first : first + 1], gate[:, first + 1 : first + 2])


def merge(out, rows):
    low = low_lanes((rows, LANES))
    return jnp.where(low, pltpu.roll(out[:rows], HEAD_DIM, 1), out[rows:])


def layer_kernel(
    chosen_ref,
    gain_ref,
    ke_ref,
    ko_ref,
    ve_ref,
    vo_ref,
    lo_ref,
    hi_hbm,
    tok_hbm,
    wq_hbm,
    wsk_hbm,
    wsv_hbm,
    wck_hbm,
    wcv_hbm,
    wg_hbm,
    ki_hbm,
    vi_hbm,
    wo_hbm,
    out_ref,
    hi,
    tok,
    wq,
    raw,
    wt,
    ki,
    vi,
    wo,
    held,
    near,
    far,
    stage,
    got,
    qp,
    qt,
    ckv,
    gate,
    scales,
    sums,
    oc,
    mix,
    heard,
    pick_vm,
    pick_sm,
    near_sm,
    tok_sem,
    local_sem,
    span_send,
    span_recv,
    send_sem,
    recv_sem,
    sum_send,
    sum_recv,
    mix_send,
    mix_recv,
):
    me, rank = lax.axis_index("kv"), lax.axis_index("tp")
    z, x = me // ACROSS, me % ACROSS
    rows, width = tok.shape
    tile = 512
    tiles = rows // tile
    q_blocks = rows // Q_BLOCK
    span = rows // SEL_BLOCK
    blocks = rows // CMP_BLOCK
    scale = HEAD_DIM ** (-0.5)

    sums[...] = jnp.zeros_like(sums)
    barrier = pltpu.get_barrier_semaphore()
    for d in range(1, OWNERS):
        pl.semaphore_signal(barrier, inc=1, device_id={"kv": (me + d) % OWNERS}, device_id_type=MESH)
    for d in range(1, RANKS):
        pl.semaphore_signal(barrier, inc=1, device_id={"tp": (rank + d) % RANKS}, device_id_type=MESH)

    loads = [
        (wq_hbm, wq),
        (wsk_hbm, raw.at[pl.ds(0, 64)]),
        (wsv_hbm, raw.at[pl.ds(64, 64)]),
        (wck_hbm, raw.at[pl.ds(128, 64)]),
        (wcv_hbm, raw.at[pl.ds(192, 64)]),
        (wg_hbm, raw.at[pl.ds(256, 32)]),
        (hi_hbm.at[pl.ds(pl.multiple_of(me * span, span), span)], hi),
        (ki_hbm, ki),
        (vi_hbm, vi),
        (wo_hbm, wo),
    ]
    copies = [pltpu.make_async_copy(a, b, local_sem.at[n]) for n, (a, b) in enumerate(loads)]
    tok_copies = [
        pltpu.make_async_copy(tok_hbm.at[pl.ds(n * tile, tile)], tok.at[pl.ds(n * tile, tile)], tok_sem.at[n])
        for n in range(tiles)
    ]
    for copy in copies[:7]:
        copy.start()
    for copy in tok_copies:
        copy.start()
    for copy in copies[7:]:
        copy.start()

    chosen = chosen_ref[...]
    near_owner, far_owner = lax.rem(me + OWNERS - ACROSS, OWNERS), x
    line = lax.broadcasted_iota(jnp.int32, chosen.shape, 0)
    index = jnp.zeros(chosen.shape, jnp.int32)
    for kind, owner in ((OWN, me), (NEAR, near_owner), (FAR, far_owner)):
        inside = jnp.where(chosen // span == owner, chosen % span, 0)
        index = jnp.where(line == kind, jnp.sum(inside, axis=0, keepdims=True), index)
    pick_vm[0] = index
    pick_vm[1] = chosen
    to_smem = pltpu.make_async_copy(pick_vm.at[0], pick_sm, local_sem.at[len(loads)])
    near_smem = pltpu.make_async_copy(pick_vm.at[1], near_sm, local_sem.at[len(loads) + 1])
    to_smem.start()
    near_smem.start()

    for copy in copies[:7]:
        copy.wait()

    gain = gain_ref[...].astype(jnp.float32).reshape(1, width)
    eye = (
        lax.broadcasted_iota(jnp.int32, (LANES, LANES), 0)
        == lax.broadcasted_iota(jnp.int32, (LANES, LANES), 1)
    ).astype(jnp.bfloat16)

    def weigh(source, first, count, target):
        def one(i, carry):
            r = pl.ds(pl.multiple_of(first + i * 16, 16), 16)
            t = pl.ds(pl.multiple_of(target + i * 16, 16), 16)
            wt[t] = (source[r].astype(jnp.float32) * gain).astype(jnp.bfloat16)
            return carry

        lax.fori_loop(0, count // 16, one, 0)

    weigh(raw, 0, 128, 0)
    for c in range(width // 256):
        cut = slice(c * 256, (c + 1) * 256)
        turned = nt_dot(eye, wq[cut])
        wt[128:256, cut] = (turned * gain[:, cut]).astype(jnp.bfloat16)

    first_half = lax.broadcasted_iota(jnp.int32, (1, LANES), 1) % HEAD_DIM < HEAD_DIM // 2
    quarter = HEAD_DIM // 2

    def turn(v, cosine, sine):
        swapped = jnp.where(first_half, pltpu.roll(v, LANES - quarter, 1), pltpu.roll(v, quarter, 1))
        return v * cosine + swapped * sine

    def project(i):
        at = pl.ds(i * tile, tile)
        v = tok[at]
        y = nt_dot(v, wt[0:256])
        w = v.astype(jnp.float32)
        inv = lax.rsqrt(jnp.mean(w * w, axis=-1, keepdims=True) + norm_eps)
        scales[at] = jnp.broadcast_to(inv, (tile, LANES))
        y = y * inv
        cos_lo, sin_lo = lo_ref[0:64], lo_ref[64:128]
        for g in range(tile // SEL_BLOCK):
            b = i * (tile // SEL_BLOCK) + g
            cut = slice(g * SEL_BLOCK, (g + 1) * SEL_BLOCK)
            cos_hi, sin_hi = hi[pl.ds(b, 1), 0:LANES], hi[pl.ds(b, 1), LANES : 2 * LANES]
            cosine = cos_hi * cos_lo - sin_hi * sin_lo
            sine = sin_hi * cos_lo + cos_hi * sin_lo
            sine = jnp.where(first_half, -sine, sine)
            part = y[cut, 0:LANES]
            low = low_lanes(part.shape)
            held[b] = jnp.where(low, turn(part, cosine, sine), part).astype(jnp.bfloat16)
            part = y[cut, LANES : 2 * LANES] * scale
            to = pl.ds(b * SEL_BLOCK, SEL_BLOCK)
            for ref, q in ((qp, part), (qt, turn(part, cosine, sine))):
                ref[0, to] = jnp.where(low, q, 0.0).astype(jnp.bfloat16)
                ref[1, to] = jnp.where(low, pltpu.roll(q, HEAD_DIM, 1), 0.0).astype(jnp.bfloat16)

    for i in range(tiles):
        tok_copies[i].wait()
        project(i)

    to_smem.wait()
    near_smem.wait()
    pl.semaphore_wait(barrier, OWNERS + RANKS - 2)

    def route(dz, dx):
        there = ((z + dz) % PLANES) * ACROSS + (x + dx) % ACROSS
        here = ((z - dz) % PLANES) * ACROSS + (x - dx) % ACROSS
        if dz == 0:
            return there, x + dx < ACROSS, here, x >= dx
        return there, z + dz < PLANES, here, z >= dz

    def span_copy(n):
        step, sends, target = ((1, z < 3, near), (3, z == 0, far), (2, z == 0, far))[n]
        there = lax.rem(me + step * ACROSS, OWNERS)
        copy = pltpu.make_async_remote_copy(
            src_ref=held,
            dst_ref=target,
            send_sem=span_send.at[n],
            recv_sem=span_recv.at[min(n, 1)],
            device_id={"kv": there},
            device_id_type=MESH,
        )
        return copy, sends

    def hop(n):
        kind, dx = HOPS[n]
        column = lax.rem(x + dx, ACROSS)
        back = lax.rem(x + ACROSS - dx, ACROSS)
        if kind == OWN:
            owner, source, sends, gets = me, held, x + dx < ACROSS, x >= dx
        elif kind == NEAR:
            owner, source, sends, gets = near_owner, near, z >= 1, z >= 1
        elif kind == FAR:
            owner, source, sends, gets = far_owner, far, z >= 2, z >= 2
        else:
            owner, source, sends, gets = me, held, z == 1, z == 3
        there = (3 if kind == SKIP else z) * ACROSS + column
        copy = pltpu.make_async_remote_copy(
            src_ref=stage.at[n],
            dst_ref=got.at[owner],
            send_sem=send_sem.at[n],
            recv_sem=recv_sem.at[n],
            device_id={"kv": there},
            device_id_type=MESH,
        )
        return copy, there, source, sends, gets

    def gather(source, kind, target, first):
        def one(j, carry):
            target[j] = source[pick_sm[kind, first + j]]
            return carry

        lax.fori_loop(0, q_blocks, one, 0)

    def send_hops(*kinds):
        for n, (kind, dx) in enumerate(HOPS):
            if kind in kinds:
                copy, there, source, sends, _ = hop(n)

                def go(n=n, kind=kind, copy=copy, there=there, source=source):
                    gather(source, OWN if kind == SKIP else kind, stage.at[n], there * q_blocks)
                    copy.start()

                pl.when(sends)(go)

    for n in range(3):
        copy, sends = span_copy(n)
        pl.when(sends)(copy.start)
    send_hops(SKIP)
    send_hops(OWN)

    weigh(raw, 128, 160, 256)

    def project_more(i, carry):
        at = pl.ds(pl.multiple_of(i * tile, tile), tile)
        y = nt_dot(tok[at], wt[256:416])
        inv = scales[at]
        ckv[at] = (y[:, 0:LANES] * inv).astype(jnp.bfloat16).astype(jnp.float32)
        gate[at] = jax.nn.sigmoid(y[:, LANES : LANES + 32] * inv[:, 0:32])
        return carry

    lax.fori_loop(0, tiles, project_more, 0)
    for copy in copies[7:9]:
        copy.wait()

    low = low_lanes((blocks, LANES))

    def summarize(is_value, e_ref, i_ref, o_ref):
        parts = []
        embed = e_ref[...].astype(jnp.float32)
        for c in range(0, CMP_BLOCK, 2):
            a = ckv[pl.ds(c, blocks, stride=CMP_BLOCK), :]
            b = ckv[pl.ds(c + 1, blocks, stride=CMP_BLOCK), :]
            if is_value:
                pair = jnp.where(low, pltpu.roll(a, HEAD_DIM, 1), b)
            else:
                pair = jnp.where(low, a, pltpu.roll(b, HEAD_DIM, 1))
            e = jnp.concatenate([embed[c : c + 1], embed[c + 1 : c + 2]], axis=1)
            parts.append((pair + e).astype(jnp.bfloat16))
        flat = jnp.concatenate(parts, axis=1)
        hidden = jax.nn.gelu(nt_dot(flat, i_ref[...])).astype(jnp.bfloat16)
        return jnp.dot(hidden, o_ref[...], preferred_element_type=jnp.float32)

    sk = summarize(False, ke_ref, ki, ko_ref)
    sv = summarize(True, ve_ref, vi, vo_ref)
    sums[me] = jnp.concatenate([sk, sv], axis=1).astype(jnp.bfloat16)

    def sum_copy(n, owner):
        there, sends, here, gets = route(*MOVES[n])
        copy = pltpu.make_async_remote_copy(
            src_ref=sums.at[owner],
            dst_ref=sums.at[owner],
            send_sem=sum_send.at[n],
            recv_sem=sum_recv.at[n],
            device_id={"kv": there},
            device_id_type=MESH,
        )
        return copy, here, sends, gets

    for n in range(len(MOVES)):
        copy, _, sends, _ = sum_copy(n, me)
        pl.when(sends)(copy.start)
    gather(held, OWN, got.at[me], me * q_blocks)

    def pass_near():
        span_copy(0)[0].wait_recv()
        send_hops(NEAR)
        gather(near, NEAR, got.at[near_owner], me * q_blocks)

    def pass_far():
        span_copy(1)[0].wait_recv()
        send_hops(FAR)
        gather(far, FAR, got.at[far_owner], me * q_blocks)

    pl.when(z >= 1)(pass_near)
    pl.when(z == 3)(pass_far)
    for n in range(len(MOVES)):
        _, here, _, gets = sum_copy(n, me)
        copy, _, _, _ = sum_copy(n, here)
        pl.when(gets)(copy.wait_recv)

    part = 256

    def compress(i, carry):
        at = pl.ds(pl.multiple_of(i * part, part), part)
        row = lax.broadcasted_iota(jnp.int32, (2 * part, 1), 0)
        pos = me * rows + i * part + jnp.where(row >= part, row - part, row)
        lane = lax.broadcasted_iota(jnp.int32, (1, OWNERS * blocks), 1)
        allowed = (lane + 1) * CMP_BLOCK - 1 <= pos
        keys = jnp.concatenate([sums[s] for s in range(OWNERS)], axis=0)
        q = jnp.concatenate([qp[0, at], qp[1, at]], axis=0)
        s = jnp.where(allowed, nt_dot(q, keys), MASKED)
        top = jnp.max(s, axis=-1, keepdims=True)
        e = jnp.exp(s - top)
        total = jnp.sum(e, axis=-1, keepdims=True)
        o = jnp.dot(e.astype(jnp.bfloat16), keys, preferred_element_type=jnp.float32)
        o = o * jnp.where(pos >= CMP_BLOCK - 1, 1.0 / total, 0.0)
        o = merge(o, part)
        g = pltpu.roll(pltpu_pad(gate[at]), LANES - 2 * rank, 1)
        oc[at] = o * gate_lanes(g, 0, o.shape)
        return carry

    def pltpu_pad(g):
        return jnp.concatenate([g, g, g, g], axis=1)

    lax.fori_loop(0, 3, compress, 0)
    pl.when(z == 2)(pass_far)
    lax.fori_loop(3, rows // part, compress, 0)

    rank_rows = rows // RANKS
    group = rank_rows // Q_BLOCK

    def mix_copy(step):
        target = (rank + 1 + step) % RANKS
        at = pl.ds(pl.multiple_of(target * rank_rows, rank_rows), rank_rows)
        return pltpu.make_async_remote_copy(
            src_ref=mix.at[at],
            dst_ref=heard.at[rank],
            send_sem=mix_send.at[step],
            recv_sem=mix_recv.at[step],
            device_id={"tp": target},
            device_id_type=MESH,
        )

    for n in range(len(HOPS)):
        copy, _, _, _, gets = hop(n)
        pl.when(gets)(copy.wait_recv)

    def choose(step, carry):
        target = (rank + 1 + step) % RANKS
        for u in range(group):
            j = target * group + u
            at = pl.ds(pl.multiple_of(j * Q_BLOCK, Q_BLOCK), Q_BLOCK)
            own = j * (Q_BLOCK // SEL_BLOCK)
            parts = [held[own + b] for b in range(Q_BLOCK // SEL_BLOCK)]
            first = me * span + own
            biases = []
            for a in range(FAR_PICKS):
                pick = near_sm[a, me * q_blocks + j]
                usable = pick < first
                owner = jnp.where(usable, pick // span, me)
                parts.append(got[owner, j])
                biases.append(jnp.where(usable, 0.0, MASKED))
            keys = jnp.concatenate(parts, axis=0)
            q = jnp.concatenate([qt[0, at], qt[1, at]], axis=0)
            s = nt_dot(q, keys)
            row = lax.broadcasted_iota(jnp.int32, (2 * Q_BLOCK, Q_BLOCK), 0)
            row = jnp.where(row >= Q_BLOCK, row - Q_BLOCK, row)
            lane = lax.broadcasted_iota(jnp.int32, row.shape, 1)
            pieces = [jnp.where(lane > row, MASKED, s[:, :Q_BLOCK])]
            low = lax.broadcasted_iota(jnp.int32, (1, LANES), 1) < SEL_BLOCK
            for a in range(0, FAR_PICKS, 2):
                c = Q_BLOCK + a * SEL_BLOCK
                pieces.append(s[:, c : c + LANES] + jnp.where(low, biases[a], biases[a + 1]))
            s = jnp.concatenate(pieces, axis=1)
            top = jnp.max(s, axis=-1, keepdims=True)
            e = jnp.exp(s - top)
            total = jnp.sum(e, axis=-1, keepdims=True)
            o = jnp.dot(e.astype(jnp.bfloat16), keys, preferred_element_type=jnp.float32)
            o = merge(o * (1.0 / total), Q_BLOCK)
            g = pltpu.roll(pltpu_pad(gate[at]), LANES - 2 * rank, 1)
            mix[at] = (oc[at] + o * gate_lanes(g, 16, o.shape)).astype(jnp.bfloat16)
        pl.when(step > 0)(lambda: mix_copy(step - 1).start())
        return carry

    lax.fori_loop(0, RANKS, choose, 0)

    own_at = pl.ds(pl.multiple_of(rank * rank_rows, rank_rows), rank_rows)
    heard[rank] = mix[own_at]
    for n in range(len(MOVES)):
        copy, _, sends, _ = sum_copy(n, me)
        pl.when(sends)(copy.wait_send)
    for n in range(len(HOPS)):
        copy, _, _, sends, _ = hop(n)
        pl.when(sends)(copy.wait_send)
    for n in range(3):
        copy, sends = span_copy(n)
        pl.when(sends)(copy.wait_send)
    copies[9].wait()
    for step in range(RANKS - 1):
        mix_copy(step).wait_send()
        mix_copy(step).wait_recv()

    lhs = jnp.concatenate([heard[t] for t in range(RANKS)], axis=1)

    def finish(c, carry):
        at = pl.ds(pl.multiple_of(c * 512, 512), 512)
        out_ref[:, at] = jnp.dot(lhs, wo[:, at], preferred_element_type=jnp.float32).astype(jnp.bfloat16)
        return carry

    lax.fori_loop(0, width // 512, finish, 0)


def rope_tables(length):
    half = HEAD_DIM // 2
    inverse = ROPE_BASE ** (-(np.arange(half, dtype=np.float32)) / np.float32(half))
    inverse = np.tile(inverse.astype(np.float32).astype(np.float64), LANES // half)

    def table(positions):
        angle = positions.astype(np.float64)[:, None] * inverse[None, :]
        return np.cos(angle), np.sin(angle)

    low = np.concatenate(table(np.arange(SEL_BLOCK)), axis=0).astype(np.float32)
    high = np.concatenate(table(np.arange(length // SEL_BLOCK) * SEL_BLOCK), axis=1).astype(np.float32)
    return jnp.asarray(low), jnp.asarray(high)


def per_device(
    tokens,
    norm_gain,
    query_weight,
    cmp_key_weight,
    cmp_value_weight,
    sel_key_weight,
    sel_value_weight,
    branch_weight,
    key_embed,
    key_inner,
    key_outer,
    value_embed,
    value_inner,
    value_outer,
    out_weight,
    chosen,
):
    rows, width = tokens.shape
    f32, bf16 = jnp.float32, jnp.bfloat16
    low, high = rope_tables(rows * OWNERS)
    span = rows // SEL_BLOCK
    q_blocks = rows // Q_BLOCK
    blocks = rows // CMP_BLOCK
    rank_rows = rows // RANKS
    picks = chosen.shape[1]
    operands = (
        chosen[0].T,
        norm_gain,
        key_embed[0],
        key_outer[0],
        value_embed[0],
        value_outer[0],
        low,
        high,
        tokens,
        query_weight,
        sel_key_weight.T,
        sel_value_weight.T,
        cmp_key_weight.T,
        cmp_value_weight.T,
        branch_weight.transpose(0, 2, 1).reshape(32, width),
        key_inner[0].T,
        value_inner[0].T,
        out_weight,
    )
    vmem = pl.BlockSpec(memory_space=pltpu.VMEM)
    hbm = pl.BlockSpec(memory_space=pl.ANY)
    dma = pltpu.SemaphoreType.DMA
    moves = len(MOVES)
    return pl.pallas_call(
        layer_kernel,
        in_specs=[vmem] * 7 + [hbm] * 11,
        out_specs=vmem,
        out_shape=jax.ShapeDtypeStruct((rank_rows, width), bf16),
        scratch_shapes=[
            pltpu.VMEM((span, 2 * LANES), f32),
            pltpu.VMEM((rows, width), bf16),
            pltpu.VMEM((width, LANES), bf16),
            pltpu.VMEM((288, width), bf16),
            pltpu.VMEM((416, width), bf16),
            pltpu.VMEM((HEAD_DIM, width), bf16),
            pltpu.VMEM((HEAD_DIM, width), bf16),
            pltpu.VMEM(out_weight.shape, bf16),
            pltpu.VMEM((span, SEL_BLOCK, LANES), bf16),
            pltpu.VMEM((span, SEL_BLOCK, LANES), bf16),
            pltpu.VMEM((span, SEL_BLOCK, LANES), bf16),
            pltpu.VMEM((len(HOPS), q_blocks, SEL_BLOCK, LANES), bf16),
            pltpu.VMEM((OWNERS, q_blocks, SEL_BLOCK, LANES), bf16),
            pltpu.VMEM((2, rows, LANES), bf16),
            pltpu.VMEM((2, rows, LANES), bf16),
            pltpu.VMEM((rows, LANES), f32),
            pltpu.VMEM((rows, 32), f32),
            pltpu.VMEM((rows, LANES), f32),
            pltpu.VMEM((OWNERS, blocks, LANES), bf16),
            pltpu.VMEM((rows, LANES), f32),
            pltpu.VMEM((rows, LANES), bf16),
            pltpu.VMEM((RANKS, rank_rows, LANES), bf16),
            pltpu.VMEM((2, FAR_PICKS, picks), jnp.int32),
            pltpu.SMEM((FAR_PICKS, picks), jnp.int32),
            pltpu.SMEM((FAR_PICKS, picks), jnp.int32),
            dma((rows // 512,)),
            dma((12,)),
            dma((3,)),
            dma((2,)),
            dma((len(HOPS),)),
            dma((len(HOPS),)),
            dma((moves,)),
            dma((moves,)),
            dma((RANKS,)),
            dma((RANKS,)),
        ],
        compiler_params=pltpu.CompilerParams(
            collective_id=0, has_side_effects=True, vmem_limit_bytes=60 * 1024 * 1024
        ),
        cost_estimate=pl.CostEstimate(flops=int(4e10), bytes_accessed=int(2e7), transcendentals=0),
        name="layer",
    )(*operands)


def solution(mesh):
    placed = (
        P("kv", None),
        P(),
        P(None, "tp"),
        P(None, "tp"),
        P(None, "tp"),
        P(None, "tp"),
        P(None, "tp"),
        P(),
        P("tp", None, None),
        P("tp", None, None),
        P("tp", None, None),
        P("tp", None, None),
        P("tp", None, None),
        P("tp", None, None),
        P(),
        P("tp", None, None),
    )
    return jax.shard_map(
        per_device, mesh=mesh, in_specs=placed, out_specs=P(("kv", "tp"), None), check_vma=False
    )
```

```python
import math

import jax
import jax.numpy as jnp
import numpy as np
from jax import lax
from jax.experimental import pallas as pl
from jax.experimental.pallas import tpu as pltpu
from jax.sharding import PartitionSpec as P

HEAD_DIM = 64
CMP_BLOCK = 32
SEL_BLOCK = 64
Q_BLOCK = 128
FAR_PICKS = 8
LANES = 2 * HEAD_DIM
PLANES = 4
ACROSS = 4
OWNERS = PLANES * ACROSS
RANKS = 8
MESH = pl.DeviceIdType.MESH

ROPE_BASE = 10000.0
norm_eps = 1e-06
MASKED = -1e30

MOVES = [(dz, dx) for dx in (2, 1, 3, 0) for dz in (2, 1, 3, 0) if (dz, dx) != (0, 0)]
OWN, NEAR, FAR, SKIP = range(4)
HOPS = [(kind, dx) for kind in (OWN, NEAR, FAR) for dx in (2, 1, 3)] + [(SKIP, dx) for dx in (0, 1, 3, 2)]


def nt_dot(a, b):
    return lax.dot_general(a, b, (((1,), (1,)), ((), ())), preferred_element_type=jnp.float32)


def low_lanes(shape):
    return lax.broadcasted_iota(jnp.int32, shape, 1) < HEAD_DIM


def gate_lanes(gate, first, shape):
    return jnp.where(low_lanes(shape), gate[:, first : first + 1], gate[:, first + 1 : first + 2])


def merge(out, rows):
    low = low_lanes((rows, LANES))
    return jnp.where(low, pltpu.roll(out[:rows], HEAD_DIM, 1), out[rows:])


def layer_kernel(
    chosen_ref,
    gain_ref,
    ke_ref,
    ko_ref,
    ve_ref,
    vo_ref,
    lo_ref,
    hi_hbm,
    tok_hbm,
    wq_hbm,
    wsk_hbm,
    wsv_hbm,
    wck_hbm,
    wcv_hbm,
    wg_hbm,
    ki_hbm,
    vi_hbm,
    wo_hbm,
    out_ref,
    hi,
    tok,
    wq,
    raw,
    wt,
    ki,
    vi,
    wo,
    held,
    near,
    far,
    stage,
    got,
    qp,
    qt,
    ckv,
    gate,
    scales,
    sums,
    keys,
    values,
    oc,
    mix,
    heard,
    pick_vm,
    pick_sm,
    near_sm,
    tok_sem,
    local_sem,
    span_send,
    span_recv,
    send_sem,
    recv_sem,
    sum_send,
    sum_recv,
    mix_send,
    mix_recv,
):
    me, rank = lax.axis_index("kv"), lax.axis_index("tp")
    z, x = me // ACROSS, me % ACROSS
    rows, width = tok.shape
    tile = 512
    tiles = rows // tile
    q_blocks = rows // Q_BLOCK
    span = rows // SEL_BLOCK
    blocks = rows // CMP_BLOCK
    scale = HEAD_DIM ** (-0.5) * math.log2(math.e)

    sums[...] = jnp.zeros_like(sums)
    barrier = pltpu.get_barrier_semaphore()
    for d in range(1, OWNERS):
        pl.semaphore_signal(barrier, inc=1, device_id={"kv": (me + d) % OWNERS}, device_id_type=MESH)
    for d in range(1, RANKS):
        pl.semaphore_signal(barrier, inc=1, device_id={"tp": (rank + d) % RANKS}, device_id_type=MESH)

    loads = [
        (wq_hbm, wq),
        (wsk_hbm, raw.at[pl.ds(0, 64)]),
        (wsv_hbm, raw.at[pl.ds(64, 64)]),
        (wck_hbm, raw.at[pl.ds(128, 64)]),
        (wcv_hbm, raw.at[pl.ds(192, 64)]),
        (wg_hbm, raw.at[pl.ds(256, 32)]),
        (hi_hbm.at[pl.ds(pl.multiple_of(me * span, span), span)], hi),
        (ki_hbm, ki),
        (vi_hbm, vi),
        (wo_hbm, wo),
    ]
    copies = [pltpu.make_async_copy(a, b, local_sem.at[n]) for n, (a, b) in enumerate(loads)]
    tok_copies = [
        pltpu.make_async_copy(tok_hbm.at[pl.ds(n * tile, tile)], tok.at[pl.ds(n * tile, tile)], tok_sem.at[n])
        for n in range(tiles)
    ]
    for copy in copies[:7]:
        copy.start()
    for copy in tok_copies:
        copy.start()
    for copy in copies[7:]:
        copy.start()

    chosen = chosen_ref[...]
    near_owner, far_owner = jnp.where(z == 0, me + ACROSS, me - ACROSS), x
    line = lax.broadcasted_iota(jnp.int32, chosen.shape, 0)
    index = jnp.zeros(chosen.shape, jnp.int32)
    for kind, owner in ((OWN, me), (NEAR, near_owner), (FAR, far_owner)):
        inside = jnp.where(chosen // span == owner, chosen % span, 0)
        index = jnp.where(line == kind, jnp.sum(inside, axis=0, keepdims=True), index)
    pick_vm[0] = index
    pick_vm[1] = chosen
    to_smem = pltpu.make_async_copy(pick_vm.at[0], pick_sm, local_sem.at[len(loads)])
    near_smem = pltpu.make_async_copy(pick_vm.at[1], near_sm, local_sem.at[len(loads) + 1])
    to_smem.start()
    near_smem.start()

    for copy in copies[:7]:
        copy.wait()

    gain = gain_ref[...].astype(jnp.float32).reshape(1, width)
    eye = (
        lax.broadcasted_iota(jnp.int32, (LANES, LANES), 0)
        == lax.broadcasted_iota(jnp.int32, (LANES, LANES), 1)
    ).astype(jnp.bfloat16)

    def weigh(source, first, count, target):
        def one(i, carry):
            r = pl.ds(pl.multiple_of(first + i * 16, 16), 16)
            t = pl.ds(pl.multiple_of(target + i * 16, 16), 16)
            wt[t] = (source[r].astype(jnp.float32) * gain).astype(jnp.bfloat16)
            return carry

        lax.fori_loop(0, count // 16, one, 0)

    weigh(raw, 0, 128, 0)
    for c in range(width // 256):
        cut = slice(c * 256, (c + 1) * 256)
        turned = nt_dot(eye, wq[cut])
        wt[128:256, cut] = (turned * gain[:, cut]).astype(jnp.bfloat16)

    first_half = lax.broadcasted_iota(jnp.int32, (1, LANES), 1) % HEAD_DIM < HEAD_DIM // 2
    flag = (lax.broadcasted_iota(jnp.int32, (1, LANES), 1) == HEAD_DIM).astype(jnp.float32)
    quarter = HEAD_DIM // 2

    def turn(v, cosine, sine):
        swapped = jnp.where(first_half, pltpu.roll(v, LANES - quarter, 1), pltpu.roll(v, quarter, 1))
        return v * cosine + swapped * sine

    def project(i):
        at = pl.ds(i * tile, tile)
        v = tok[at]
        y = nt_dot(v, wt[0:256])
        w = v.astype(jnp.float32)
        inv = lax.rsqrt(jnp.mean(w * w, axis=-1, keepdims=True) + norm_eps)
        scales[at] = jnp.broadcast_to(inv, (tile, LANES))
        y = y * inv
        cos_lo, sin_lo = lo_ref[0:64], lo_ref[64:128]
        for g in range(tile // SEL_BLOCK):
            b = i * (tile // SEL_BLOCK) + g
            cut = slice(g * SEL_BLOCK, (g + 1) * SEL_BLOCK)
            cos_hi, sin_hi = hi[pl.ds(b, 1), 0:LANES], hi[pl.ds(b, 1), LANES : 2 * LANES]
            cosine = cos_hi * cos_lo - sin_hi * sin_lo
            sine = sin_hi * cos_lo + cos_hi * sin_lo
            sine = jnp.where(first_half, -sine, sine)
            part = y[cut, 0:LANES]
            low = low_lanes(part.shape)
            held[b] = jnp.where(low, turn(part, cosine, sine), part).astype(jnp.bfloat16)
            part = y[cut, LANES : 2 * LANES] * scale
            to = pl.ds(b * SEL_BLOCK, SEL_BLOCK)
            for ref, q, rest in ((qp, part, flag), (qt, turn(part, cosine, sine), 0.0)):
                ref[0, to] = jnp.where(low, q, rest).astype(jnp.bfloat16)
                ref[1, to] = jnp.where(low, pltpu.roll(q, HEAD_DIM, 1), rest).astype(jnp.bfloat16)

    for i in range(tiles):
        tok_copies[i].wait()
        project(i)

    to_smem.wait()
    near_smem.wait()
    pl.semaphore_wait(barrier, OWNERS + RANKS - 2)

    def route(dz, dx):
        there = ((z + dz) % PLANES) * ACROSS + (x + dx) % ACROSS
        here = ((z - dz) % PLANES) * ACROSS + (x - dx) % ACROSS
        if dz == 0:
            return there, x + dx < ACROSS, here, x >= dx
        return there, z + dz < PLANES, here, z >= dz

    def span_copy(n):
        step, sends, source, target = (
            (1, z < 3, held, near),
            (3, z == 1, held, near),
            (3, z == 0, held, far),
            (3, z == 3, far, far),
        )[n]
        return (
            pltpu.make_async_remote_copy(
                src_ref=source,
                dst_ref=target,
                send_sem=span_send.at[n],
                recv_sem=span_recv.at[n // 2],
                device_id={"kv": lax.rem(me + step * ACROSS, OWNERS)},
                device_id_type=MESH,
            ),
            sends,
        )

    def hop(n):
        kind, dx = HOPS[n]
        column = lax.rem(x + dx, ACROSS)
        back = lax.rem(x + ACROSS - dx, ACROSS)
        if kind == OWN:
            owner, source, sends, gets = me, held, x + dx < ACROSS, x >= dx
        elif kind == NEAR:
            owner, source, sends, gets = near_owner, near, z >= 1, z >= 1
        elif kind == FAR:
            owner, source, sends, gets = far_owner, far, z >= 2, z >= 2
        else:
            owner, source, sends, gets = near_owner, near, z == 0, z == 3
        there = (3 if kind == SKIP else z) * ACROSS + column
        copy = pltpu.make_async_remote_copy(
            src_ref=stage.at[n],
            dst_ref=got.at[owner],
            send_sem=send_sem.at[n],
            recv_sem=recv_sem.at[n],
            device_id={"kv": there},
            device_id_type=MESH,
        )
        return copy, there, source, sends, gets

    def gather(source, kind, target, first):
        def one(j, carry):
            target[j] = source[pick_sm[kind, first + j]]
            return carry

        lax.fori_loop(0, q_blocks, one, 0)

    def send_hops(*kinds):
        for n, (kind, dx) in enumerate(HOPS):
            if kind in kinds:
                copy, there, source, sends, _ = hop(n)

                def go(n=n, kind=kind, copy=copy, there=there, source=source):
                    gather(source, NEAR if kind == SKIP else kind, stage.at[n], there * q_blocks)
                    copy.start()

                pl.when(sends)(go)

    for n in range(3):
        copy, sends = span_copy(n)
        pl.when(sends)(copy.start)
    send_hops(OWN)

    weigh(raw, 128, 160, 256)

    def project_more(i, carry):
        at = pl.ds(pl.multiple_of(i * tile, tile), tile)
        y = nt_dot(tok[at], wt[256:416])
        inv = scales[at]
        ckv[at] = (y[:, 0:LANES] * inv).astype(jnp.bfloat16).astype(jnp.float32)
        gate[at] = jax.nn.sigmoid(y[:, LANES : LANES + 32] * inv[:, 0:32])
        return carry

    lax.fori_loop(0, tiles, project_more, 0)
    for copy in copies[7:9]:
        copy.wait()

    low = low_lanes((blocks, LANES))

    def summarize(is_value, e_ref, i_ref, o_ref):
        parts = []
        embed = e_ref[...].astype(jnp.float32)
        for c in range(0, CMP_BLOCK, 2):
            a = ckv[pl.ds(c, blocks, stride=CMP_BLOCK), :]
            b = ckv[pl.ds(c + 1, blocks, stride=CMP_BLOCK), :]
            if is_value:
                pair = jnp.where(low, pltpu.roll(a, HEAD_DIM, 1), b)
            else:
                pair = jnp.where(low, a, pltpu.roll(b, HEAD_DIM, 1))
            e = jnp.concatenate([embed[c : c + 1], embed[c + 1 : c + 2]], axis=1)
            parts.append((pair + e).astype(jnp.bfloat16))
        flat = jnp.concatenate(parts, axis=1)
        hidden = jax.nn.gelu(nt_dot(flat, i_ref[...])).astype(jnp.bfloat16)
        return jnp.dot(hidden, o_ref[...], preferred_element_type=jnp.float32)

    sk = summarize(False, ke_ref, ki, ko_ref)
    sv = summarize(True, ve_ref, vi, vo_ref)
    sums[me] = jnp.concatenate([sk, sv], axis=1).astype(jnp.bfloat16)

    def sum_copy(n, owner):
        there, sends, here, gets = route(*MOVES[n])
        copy = pltpu.make_async_remote_copy(
            src_ref=sums.at[owner],
            dst_ref=sums.at[owner],
            send_sem=sum_send.at[n],
            recv_sem=sum_recv.at[n],
            device_id={"kv": there},
            device_id_type=MESH,
        )
        return copy, here, sends, gets

    for n in range(len(MOVES)):
        copy, _, sends, _ = sum_copy(n, me)
        pl.when(sends)(copy.start)
    gather(held, OWN, got.at[me], me * q_blocks)

    def pass_near():
        send_hops(NEAR)
        gather(near, NEAR, got.at[near_owner], me * q_blocks)

    def pass_far():
        span_copy(2)[0].wait_recv()
        copy, sends = span_copy(3)
        pl.when(sends)(copy.start)
        send_hops(FAR)
        gather(far, FAR, got.at[far_owner], me * q_blocks)

    span_copy(0)[0].wait_recv()
    send_hops(SKIP)
    pl.when(z >= 1)(pass_near)
    pl.when(z == 3)(pass_far)
    for n in range(len(MOVES)):
        _, here, _, gets = sum_copy(n, me)
        copy, _, _, _ = sum_copy(n, here)
        pl.when(gets)(copy.wait_recv)

    lane = lax.broadcasted_iota(jnp.int32, (blocks, LANES), 1)
    for d in range(OWNERS):
        owner = lax.rem(me + d, OWNERS)
        both = sums[owner]
        bar = jnp.where(owner > me, MASKED, 0.0).astype(jnp.bfloat16)
        rows_at = slice(d * blocks, (d + 1) * blocks)
        keys[rows_at] = jnp.where(lane == HEAD_DIM, bar, both)
        values[rows_at] = jnp.where(lane < HEAD_DIM, jnp.ones_like(both), both)

    part = 256

    def compress(i, carry):
        at = pl.ds(pl.multiple_of(i * part, part), part)
        row = lax.broadcasted_iota(jnp.int32, (2 * part, 1), 0)
        pos = i * part + jnp.where(row >= part, row - part, row)
        lane = lax.broadcasted_iota(jnp.int32, (1, LANES), 1)
        q = jnp.concatenate([qp[0, at], qp[1, at]], axis=0)
        s = nt_dot(q, keys[...])
        own = jnp.where((lane >= blocks) | ((lane + 1) * CMP_BLOCK - 1 <= pos), s[:, :LANES], MASKED)
        s = jnp.concatenate([own, s[:, LANES:]], axis=1)
        e = jnp.exp2(s - jnp.max(s, axis=-1, keepdims=True))
        o = jnp.dot(e.astype(jnp.bfloat16), values[...], preferred_element_type=jnp.float32)
        o = jnp.where(me * rows + pos >= CMP_BLOCK - 1, o * pltpu.roll(1.0 / o, HEAD_DIM, 1), 0.0)
        o = merge(o, part)
        g = pltpu.roll(pltpu_pad(gate[at]), LANES - 2 * rank, 1)
        oc[at] = o * gate_lanes(g, 0, o.shape)
        return carry

    def pltpu_pad(g):
        return jnp.concatenate([g, g, g, g], axis=1)

    lax.fori_loop(0, 3, compress, 0)
    pl.when(z == 2)(pass_far)
    lax.fori_loop(3, rows // part, compress, 0)

    rank_rows = rows // RANKS
    group = rank_rows // Q_BLOCK

    def mix_copy(step):
        target = (rank + 1 + step) % RANKS
        at = pl.ds(pl.multiple_of(target * rank_rows, rank_rows), rank_rows)
        return pltpu.make_async_remote_copy(
            src_ref=mix.at[at],
            dst_ref=heard.at[rank],
            send_sem=mix_send.at[step],
            recv_sem=mix_recv.at[step],
            device_id={"tp": target},
            device_id_type=MESH,
        )

    for n in range(len(HOPS)):
        copy, _, _, _, gets = hop(n)
        pl.when(gets)(copy.wait_recv)

    def choose(step, carry):
        target = (rank + 1 + step) % RANKS
        for u in range(group):
            j = target * group + u
            at = pl.ds(pl.multiple_of(j * Q_BLOCK, Q_BLOCK), Q_BLOCK)
            own = j * (Q_BLOCK // SEL_BLOCK)
            parts = [held[own + b] for b in range(Q_BLOCK // SEL_BLOCK)]
            first = me * span + own
            biases = []
            for a in range(FAR_PICKS):
                pick = near_sm[a, me * q_blocks + j]
                usable = pick < first
                owner = jnp.where(usable, pick // span, me)
                parts.append(got[owner, j])
                biases.append(jnp.where(usable, 0.0, MASKED))
            both = jnp.concatenate(parts, axis=0)
            q = jnp.concatenate([qt[0, at], qt[1, at]], axis=0)
            s = nt_dot(q, both)
            row = lax.broadcasted_iota(jnp.int32, (2 * Q_BLOCK, Q_BLOCK), 0)
            row = jnp.where(row >= Q_BLOCK, row - Q_BLOCK, row)
            lane = lax.broadcasted_iota(jnp.int32, row.shape, 1)
            pieces = [jnp.where(lane > row, MASKED, s[:, :Q_BLOCK])]
            low = lax.broadcasted_iota(jnp.int32, (1, LANES), 1) < SEL_BLOCK
            for a in range(0, FAR_PICKS, 2):
                c = Q_BLOCK + a * SEL_BLOCK
                pieces.append(s[:, c : c + LANES] + jnp.where(low, biases[a], biases[a + 1]))
            s = jnp.concatenate(pieces, axis=1)
            top = jnp.max(s, axis=-1, keepdims=True)
            e = jnp.exp2(s - top)
            both = jnp.where(low_lanes(both.shape), jnp.ones_like(both), both)
            o = jnp.dot(e.astype(jnp.bfloat16), both, preferred_element_type=jnp.float32)
            o = merge(o * pltpu.roll(1.0 / o, HEAD_DIM, 1), Q_BLOCK)
            g = pltpu.roll(pltpu_pad(gate[at]), LANES - 2 * rank, 1)
            mix[at] = (oc[at] + o * gate_lanes(g, 16, o.shape)).astype(jnp.bfloat16)
        pl.when(step > 0)(lambda: mix_copy(step - 1).start())
        return carry

    lax.fori_loop(0, RANKS, choose, 0)

    own_at = pl.ds(pl.multiple_of(rank * rank_rows, rank_rows), rank_rows)
    heard[rank] = mix[own_at]
    for n in range(len(MOVES)):
        copy, _, sends, _ = sum_copy(n, me)
        pl.when(sends)(copy.wait_send)
    for n in range(len(HOPS)):
        copy, _, _, sends, _ = hop(n)
        pl.when(sends)(copy.wait_send)
    for n in range(4):
        copy, sends = span_copy(n)
        pl.when(sends)(copy.wait_send)
    copies[9].wait()
    for step in range(RANKS - 1):
        mix_copy(step).wait_send()
        mix_copy(step).wait_recv()

    lhs = jnp.concatenate([heard[t] for t in range(RANKS)], axis=1)

    def finish(c, carry):
        at = pl.ds(pl.multiple_of(c * 512, 512), 512)
        out_ref[:, at] = jnp.dot(lhs, wo[:, at], preferred_element_type=jnp.float32).astype(jnp.bfloat16)
        return carry

    lax.fori_loop(0, width // 512, finish, 0)


def rope_tables(length):
    half = HEAD_DIM // 2
    inverse = ROPE_BASE ** (-(np.arange(half, dtype=np.float32)) / np.float32(half))
    inverse = np.tile(inverse.astype(np.float32).astype(np.float64), LANES // half)

    def table(positions):
        angle = positions.astype(np.float64)[:, None] * inverse[None, :]
        return np.cos(angle), np.sin(angle)

    low = np.concatenate(table(np.arange(SEL_BLOCK)), axis=0).astype(np.float32)
    high = np.concatenate(table(np.arange(length // SEL_BLOCK) * SEL_BLOCK), axis=1).astype(np.float32)
    return jnp.asarray(low), jnp.asarray(high)


def per_device(
    tokens,
    norm_gain,
    query_weight,
    cmp_key_weight,
    cmp_value_weight,
    sel_key_weight,
    sel_value_weight,
    branch_weight,
    key_embed,
    key_inner,
    key_outer,
    value_embed,
    value_inner,
    value_outer,
    out_weight,
    chosen,
):
    rows, width = tokens.shape
    f32, bf16 = jnp.float32, jnp.bfloat16
    low, high = rope_tables(rows * OWNERS)
    span = rows // SEL_BLOCK
    q_blocks = rows // Q_BLOCK
    blocks = rows // CMP_BLOCK
    rank_rows = rows // RANKS
    picks = chosen.shape[1]
    operands = (
        chosen[0].T,
        norm_gain,
        key_embed[0],
        key_outer[0],
        value_embed[0],
        value_outer[0],
        low,
        high,
        tokens,
        query_weight,
        sel_key_weight.T,
        sel_value_weight.T,
        cmp_key_weight.T,
        cmp_value_weight.T,
        branch_weight.transpose(0, 2, 1).reshape(32, width),
        key_inner[0].T,
        value_inner[0].T,
        out_weight,
    )
    vmem = pl.BlockSpec(memory_space=pltpu.VMEM)
    hbm = pl.BlockSpec(memory_space=pl.ANY)
    dma = pltpu.SemaphoreType.DMA
    moves = len(MOVES)
    return pl.pallas_call(
        layer_kernel,
        in_specs=[vmem] * 7 + [hbm] * 11,
        out_specs=vmem,
        out_shape=pltpu.VMEM((rank_rows, width), bf16),
        scratch_shapes=[
            pltpu.VMEM((span, 2 * LANES), f32),
            pltpu.VMEM((rows, width), bf16),
            pltpu.VMEM((width, LANES), bf16),
            pltpu.VMEM((288, width), bf16),
            pltpu.VMEM((416, width), bf16),
            pltpu.VMEM((HEAD_DIM, width), bf16),
            pltpu.VMEM((HEAD_DIM, width), bf16),
            pltpu.VMEM(out_weight.shape, bf16),
            pltpu.VMEM((span, SEL_BLOCK, LANES), bf16),
            pltpu.VMEM((span, SEL_BLOCK, LANES), bf16),
            pltpu.VMEM((span, SEL_BLOCK, LANES), bf16),
            pltpu.VMEM((len(HOPS), q_blocks, SEL_BLOCK, LANES), bf16),
            pltpu.VMEM((OWNERS, q_blocks, SEL_BLOCK, LANES), bf16),
            pltpu.VMEM((2, rows, LANES), bf16),
            pltpu.VMEM((2, rows, LANES), bf16),
            pltpu.VMEM((rows, LANES), f32),
            pltpu.VMEM((rows, 32), f32),
            pltpu.VMEM((rows, LANES), f32),
            pltpu.VMEM((OWNERS, blocks, LANES), bf16),
            pltpu.VMEM((OWNERS * blocks, LANES), bf16),
            pltpu.VMEM((OWNERS * blocks, LANES), bf16),
            pltpu.VMEM((rows, LANES), f32),
            pltpu.VMEM((rows, LANES), bf16),
            pltpu.VMEM((RANKS, rank_rows, LANES), bf16),
            pltpu.VMEM((2, FAR_PICKS, picks), jnp.int32),
            pltpu.SMEM((FAR_PICKS, picks), jnp.int32),
            pltpu.SMEM((FAR_PICKS, picks), jnp.int32),
            dma((rows // 512,)),
            dma((12,)),
            dma((4,)),
            dma((2,)),
            dma((len(HOPS),)),
            dma((len(HOPS),)),
            dma((moves,)),
            dma((moves,)),
            dma((RANKS,)),
            dma((RANKS,)),
        ],
        compiler_params=pltpu.CompilerParams(
            collective_id=0, has_side_effects=True, vmem_limit_bytes=60 * 1024 * 1024
        ),
        cost_estimate=pl.CostEstimate(flops=int(4e10), bytes_accessed=int(2e7), transcendentals=0),
        name="layer",
    )(*operands)


def solution(mesh):
    placed = (
        P("kv", None),
        P(),
        P(None, "tp"),
        P(None, "tp"),
        P(None, "tp"),
        P(None, "tp"),
        P(None, "tp"),
        P(),
        P("tp", None, None),
        P("tp", None, None),
        P("tp", None, None),
        P("tp", None, None),
        P("tp", None, None),
        P("tp", None, None),
        P(),
        P("tp", None, None),
    )
    return jax.shard_map(
        per_device, mesh=mesh, in_specs=placed, out_specs=P(("kv", "tp"), None), check_vma=False
    )
```

```python
import functools
import math

import jax
import jax.numpy as jnp
import numpy as np
from jax import lax
from jax.experimental import pallas as pl
from jax.experimental.pallas import tpu as pltpu
from jax.sharding import PartitionSpec as P

HEAD_DIM = 64
CMP_BLOCK = 32
SEL_BLOCK = 64
Q_BLOCK = 128
FAR_PICKS = 8
LANES = 2 * HEAD_DIM
PLANES = 4
ACROSS = 4
OWNERS = PLANES * ACROSS
RANKS = 8
MESH = pl.DeviceIdType.MESH

ROPE_BASE = 10000.0
norm_eps = 1e-06
MASKED = -1e30

MOVES = [(dz, dx) for dx in (2, 1, 3, 0) for dz in (2, 1, 3, 0) if (dz, dx) != (0, 0)]
OWN, NEAR, FAR, SKIP = range(4)
HOPS = [(kind, dx) for kind in (OWN, NEAR, FAR) for dx in (2, 1, 3)] + [(SKIP, dx) for dx in (0, 1, 3, 2)]


def nt_dot(a, b):
    return lax.dot_general(a, b, (((1,), (1,)), ((), ())), preferred_element_type=jnp.float32)


def low_lanes(shape):
    return lax.broadcasted_iota(jnp.int32, shape, 1) < HEAD_DIM


def gate_lanes(gate, first, shape):
    return jnp.where(low_lanes(shape), gate[:, first : first + 1], gate[:, first + 1 : first + 2])


def merge(out, rows):
    low = low_lanes((rows, LANES))
    return jnp.where(low, pltpu.roll(out[:rows], HEAD_DIM, 1), out[rows:])


def layer_kernel(
    chosen_ref,
    gain_ref,
    ke_ref,
    ko_ref,
    ve_ref,
    vo_ref,
    lo_ref,
    hi_hbm,
    tok_hbm,
    wq_hbm,
    wsk_hbm,
    wsv_hbm,
    wck_hbm,
    wcv_hbm,
    wg_hbm,
    ki_hbm,
    vi_hbm,
    wo_hbm,
    out_ref,
    hi,
    tok,
    wq,
    raw,
    wt,
    ki,
    vi,
    wo,
    held,
    near,
    far,
    stage,
    got,
    qp,
    qt,
    ckv,
    gate,
    scales,
    sums,
    keys,
    values,
    oc,
    mix,
    heard,
    pick_vm,
    pick_sm,
    near_sm,
    tok_sem,
    local_sem,
    span_send,
    span_recv,
    send_sem,
    recv_sem,
    sum_send,
    sum_recv,
    mix_send,
    mix_recv,
):
    me, rank = lax.axis_index("kv"), lax.axis_index("tp")
    z, x = me // ACROSS, me % ACROSS
    rows, width = tok.shape
    tile = 512
    tiles = rows // tile
    q_blocks = rows // Q_BLOCK
    span = rows // SEL_BLOCK
    blocks = rows // CMP_BLOCK
    scale = HEAD_DIM ** (-0.5) * math.log2(math.e)

    sums[...] = jnp.zeros_like(sums)
    barrier = pltpu.get_barrier_semaphore()
    for d in range(1, OWNERS):
        pl.semaphore_signal(barrier, inc=1, device_id={"kv": (me + d) % OWNERS}, device_id_type=MESH)
    for d in range(1, RANKS):
        pl.semaphore_signal(barrier, inc=1, device_id={"tp": (rank + d) % RANKS}, device_id_type=MESH)

    loads = [
        (wq_hbm, wq),
        (wsk_hbm, raw.at[pl.ds(0, 64)]),
        (wsv_hbm, raw.at[pl.ds(64, 64)]),
        (wck_hbm, raw.at[pl.ds(128, 64)]),
        (wcv_hbm, raw.at[pl.ds(192, 64)]),
        (wg_hbm, raw.at[pl.ds(256, 32)]),
        (hi_hbm.at[pl.ds(pl.multiple_of(me * span, span), span)], hi),
        (ki_hbm, ki),
        (vi_hbm, vi),
        (wo_hbm, wo),
    ]
    copies = [pltpu.make_async_copy(a, b, local_sem.at[n]) for n, (a, b) in enumerate(loads)]
    tok_copies = [
        pltpu.make_async_copy(tok_hbm.at[pl.ds(n * tile, tile)], tok.at[pl.ds(n * tile, tile)], tok_sem.at[n])
        for n in range(tiles)
    ]
    for copy in copies[:7]:
        copy.start()
    for copy in tok_copies:
        copy.start()
    for copy in copies[7:]:
        copy.start()

    chosen = chosen_ref[...]
    near_owner, far_owner = jnp.where(z == 0, me + ACROSS, me - ACROSS), x
    line = lax.broadcasted_iota(jnp.int32, chosen.shape, 0)
    index = jnp.zeros(chosen.shape, jnp.int32)
    for kind, owner in ((OWN, me), (NEAR, near_owner), (FAR, far_owner)):
        inside = jnp.where(chosen // span == owner, chosen % span, 0)
        index = jnp.where(line == kind, jnp.sum(inside, axis=0, keepdims=True), index)
    pick_vm[0] = index
    pick_vm[1] = chosen
    to_smem = pltpu.make_async_copy(pick_vm.at[0], pick_sm, local_sem.at[len(loads)])
    near_smem = pltpu.make_async_copy(pick_vm.at[1], near_sm, local_sem.at[len(loads) + 1])
    to_smem.start()
    near_smem.start()

    for copy in copies[:7]:
        copy.wait()

    gain = gain_ref[...].astype(jnp.float32).reshape(1, width)
    eye = (
        lax.broadcasted_iota(jnp.int32, (LANES, LANES), 0)
        == lax.broadcasted_iota(jnp.int32, (LANES, LANES), 1)
    ).astype(jnp.bfloat16)

    def weigh(source, first, count, target):
        def one(i, carry):
            r = pl.ds(pl.multiple_of(first + i * 16, 16), 16)
            t = pl.ds(pl.multiple_of(target + i * 16, 16), 16)
            wt[t] = (source[r].astype(jnp.float32) * gain).astype(jnp.bfloat16)
            return carry

        lax.fori_loop(0, count // 16, one, 0)

    weigh(raw, 0, 128, 0)
    for c in range(width // 256):
        cut = slice(c * 256, (c + 1) * 256)
        turned = nt_dot(eye, wq[cut])
        wt[128:256, cut] = (turned * gain[:, cut]).astype(jnp.bfloat16)

    first_half = lax.broadcasted_iota(jnp.int32, (1, LANES), 1) % HEAD_DIM < HEAD_DIM // 2
    flag = (lax.broadcasted_iota(jnp.int32, (1, LANES), 1) == HEAD_DIM).astype(jnp.float32)
    quarter = HEAD_DIM // 2

    def turn(v, cosine, sine):
        swapped = jnp.where(first_half, pltpu.roll(v, LANES - quarter, 1), pltpu.roll(v, quarter, 1))
        return v * cosine + swapped * sine

    def project(i):
        at = pl.ds(i * tile, tile)
        v = tok[at]
        y = nt_dot(v, wt[0:256])
        w = v.astype(jnp.float32)
        inv = lax.rsqrt(jnp.mean(w * w, axis=-1, keepdims=True) + norm_eps)
        scales[at] = jnp.broadcast_to(inv, (tile, LANES))
        y = y * inv
        cos_lo, sin_lo = lo_ref[0:64], lo_ref[64:128]
        for g in range(tile // SEL_BLOCK):
            b = i * (tile // SEL_BLOCK) + g
            cut = slice(g * SEL_BLOCK, (g + 1) * SEL_BLOCK)
            cos_hi, sin_hi = hi[pl.ds(b, 1), 0:LANES], hi[pl.ds(b, 1), LANES : 2 * LANES]
            cosine = cos_hi * cos_lo - sin_hi * sin_lo
            sine = sin_hi * cos_lo + cos_hi * sin_lo
            sine = jnp.where(first_half, -sine, sine)
            part = y[cut, 0:LANES]
            low = low_lanes(part.shape)
            held[b] = jnp.where(low, turn(part, cosine, sine), part).astype(jnp.bfloat16)
            part = y[cut, LANES : 2 * LANES] * scale
            to = pl.ds(b * SEL_BLOCK, SEL_BLOCK)
            for ref, q, rest in ((qp, part, flag), (qt, turn(part, cosine, sine), 0.0)):
                ref[0, to] = jnp.where(low, q, rest).astype(jnp.bfloat16)
                ref[1, to] = jnp.where(low, pltpu.roll(q, HEAD_DIM, 1), rest).astype(jnp.bfloat16)

    for i in range(tiles):
        tok_copies[i].wait()
        project(i)

    to_smem.wait()
    near_smem.wait()
    pl.semaphore_wait(barrier, OWNERS + RANKS - 2)

    def route(dz, dx):
        there = ((z + dz) % PLANES) * ACROSS + (x + dx) % ACROSS
        here = ((z - dz) % PLANES) * ACROSS + (x - dx) % ACROSS
        if dz == 0:
            return there, x + dx < ACROSS, here, x >= dx
        return there, z + dz < PLANES, here, z >= dz

    def span_copy(n):
        step, sends, source, target = (
            (1, z < 3, held, near),
            (3, z == 1, held, near),
            (3, z == 0, held, far),
            (3, z == 3, far, far),
        )[n]
        return (
            pltpu.make_async_remote_copy(
                src_ref=source,
                dst_ref=target,
                send_sem=span_send.at[n],
                recv_sem=span_recv.at[n // 2],
                device_id={"kv": lax.rem(me + step * ACROSS, OWNERS)},
                device_id_type=MESH,
            ),
            sends,
        )

    def hop(n):
        kind, dx = HOPS[n]
        column = lax.rem(x + dx, ACROSS)
        back = lax.rem(x + ACROSS - dx, ACROSS)
        if kind == OWN:
            owner, source, sends, gets = me, held, x + dx < ACROSS, x >= dx
        elif kind == NEAR:
            owner, source, sends, gets = near_owner, near, z >= 1, z >= 1
        elif kind == FAR:
            owner, source, sends, gets = far_owner, far, z >= 2, z >= 2
        else:
            owner, source, sends, gets = near_owner, near, z == 0, z == 3
        there = (3 if kind == SKIP else z) * ACROSS + column
        copy = pltpu.make_async_remote_copy(
            src_ref=stage.at[n],
            dst_ref=got.at[owner],
            send_sem=send_sem.at[n],
            recv_sem=recv_sem.at[n],
            device_id={"kv": there},
            device_id_type=MESH,
        )
        return copy, there, source, sends, gets

    def gather(source, kind, target, first):
        def one(j, carry):
            target[j] = source[pick_sm[kind, first + j]]
            return carry

        lax.fori_loop(0, q_blocks, one, 0)

    def send_hops(*kinds):
        for n, (kind, dx) in enumerate(HOPS):
            if kind in kinds:
                copy, there, source, sends, _ = hop(n)

                def go(n=n, kind=kind, copy=copy, there=there, source=source):
                    gather(source, NEAR if kind == SKIP else kind, stage.at[n], there * q_blocks)
                    copy.start()

                pl.when(sends)(go)

    for n in range(3):
        copy, sends = span_copy(n)
        pl.when(sends)(copy.start)
    send_hops(OWN)

    weigh(raw, 128, 160, 256)

    def project_more(i, carry):
        at = pl.ds(pl.multiple_of(i * tile, tile), tile)
        y = nt_dot(tok[at], wt[256:416])
        inv = scales[at]
        ckv[at] = (y[:, 0:LANES] * inv).astype(jnp.bfloat16).astype(jnp.float32)
        gate[at] = jax.nn.sigmoid(y[:, LANES : LANES + 32] * inv[:, 0:32])
        return carry

    lax.fori_loop(0, tiles, project_more, 0)
    for copy in copies[7:9]:
        copy.wait()

    low = low_lanes((blocks, LANES))

    def summarize(is_value, e_ref, i_ref, o_ref):
        parts = []
        embed = e_ref[...].astype(jnp.float32)
        for c in range(0, CMP_BLOCK, 2):
            a = ckv[pl.ds(c, blocks, stride=CMP_BLOCK), :]
            b = ckv[pl.ds(c + 1, blocks, stride=CMP_BLOCK), :]
            if is_value:
                pair = jnp.where(low, pltpu.roll(a, HEAD_DIM, 1), b)
            else:
                pair = jnp.where(low, a, pltpu.roll(b, HEAD_DIM, 1))
            e = jnp.concatenate([embed[c : c + 1], embed[c + 1 : c + 2]], axis=1)
            parts.append((pair + e).astype(jnp.bfloat16))
        flat = jnp.concatenate(parts, axis=1)
        hidden = jax.nn.gelu(nt_dot(flat, i_ref[...])).astype(jnp.bfloat16)
        return jnp.dot(hidden, o_ref[...], preferred_element_type=jnp.float32)

    sk = summarize(False, ke_ref, ki, ko_ref)
    sv = summarize(True, ve_ref, vi, vo_ref)
    sums[me] = jnp.concatenate([sk, sv], axis=1).astype(jnp.bfloat16)

    def sum_copy(n, owner):
        there, sends, here, gets = route(*MOVES[n])
        copy = pltpu.make_async_remote_copy(
            src_ref=sums.at[owner],
            dst_ref=sums.at[owner],
            send_sem=sum_send.at[n],
            recv_sem=sum_recv.at[n],
            device_id={"kv": there},
            device_id_type=MESH,
        )
        return copy, here, sends, gets

    for n in range(len(MOVES)):
        copy, _, sends, _ = sum_copy(n, me)
        pl.when(sends)(copy.start)
    gather(held, OWN, got.at[me], me * q_blocks)

    def pass_near():
        send_hops(NEAR)
        gather(near, NEAR, got.at[near_owner], me * q_blocks)

    def hand_back():
        span_copy(2)[0].wait_recv()
        span_copy(3)[0].start()

    def pass_far():
        pl.when(z == 2)(span_copy(2)[0].wait_recv)
        send_hops(FAR)
        gather(far, FAR, got.at[far_owner], me * q_blocks)

    pl.when(z == 3)(hand_back)
    span_copy(0)[0].wait_recv()
    send_hops(SKIP)
    pl.when(z >= 1)(pass_near)
    pl.when(z == 3)(pass_far)
    for n in range(len(MOVES)):
        _, here, _, gets = sum_copy(n, me)
        copy, _, _, _ = sum_copy(n, here)
        pl.when(gets)(copy.wait_recv)

    lane = lax.broadcasted_iota(jnp.int32, (blocks, LANES), 1)
    for d in range(OWNERS):
        owner = lax.rem(me + d, OWNERS)
        both = sums[owner]
        bar = jnp.where(owner > me, MASKED, 0.0).astype(jnp.bfloat16)
        rows_at = slice(d * blocks, (d + 1) * blocks)
        keys[rows_at] = jnp.where(lane == HEAD_DIM, bar, both)
        values[rows_at] = jnp.where(lane < HEAD_DIM, jnp.ones_like(both), both)

    part = 256

    def compress(i, carry):
        at = pl.ds(pl.multiple_of(i * part, part), part)
        pos = i * part + lax.broadcasted_iota(jnp.int32, (part, 1), 0)
        lane = lax.broadcasted_iota(jnp.int32, (1, LANES), 1)
        scored = [nt_dot(qp[h, at], keys[...]) for h in range(2)]
        outs = []
        for s in scored:
            own = jnp.where((lane >= blocks) | ((lane + 1) * CMP_BLOCK - 1 <= pos), s[:, :LANES], MASKED)
            pieces = [own] + [s[:, c : c + LANES] for c in range(LANES, OWNERS * blocks, LANES)]
            top = jnp.max(functools.reduce(jnp.maximum, pieces), axis=-1, keepdims=True)
            e = jnp.concatenate([jnp.exp2(p - top).astype(jnp.bfloat16) for p in pieces], axis=1)
            o = jnp.dot(e, values[...], preferred_element_type=jnp.float32)
            outs.append(o * pltpu.roll(1.0 / o, HEAD_DIM, 1))
        o = jnp.where(low_lanes(outs[0].shape), pltpu.roll(outs[0], HEAD_DIM, 1), outs[1])
        o = jnp.where(me * rows + pos >= CMP_BLOCK - 1, o, 0.0)
        g = pltpu.roll(pltpu_pad(gate[at]), LANES - 2 * rank, 1)
        oc[at] = o * gate_lanes(g, 0, o.shape)
        return carry

    def pltpu_pad(g):
        return jnp.concatenate([g, g, g, g], axis=1)

    lax.fori_loop(0, 3, compress, 0)
    pl.when(z == 2)(pass_far)
    lax.fori_loop(3, rows // part, compress, 0)

    rank_rows = rows // RANKS
    group = rank_rows // Q_BLOCK

    def mix_copy(step):
        target = (rank + 1 + step) % RANKS
        at = pl.ds(pl.multiple_of(target * rank_rows, rank_rows), rank_rows)
        return pltpu.make_async_remote_copy(
            src_ref=mix.at[at],
            dst_ref=heard.at[rank],
            send_sem=mix_send.at[step],
            recv_sem=mix_recv.at[step],
            device_id={"tp": target},
            device_id_type=MESH,
        )

    for n in range(len(HOPS)):
        copy, _, _, _, gets = hop(n)
        pl.when(gets)(copy.wait_recv)

    own_row = lax.broadcasted_iota(jnp.int32, (2 * Q_BLOCK, Q_BLOCK), 0)
    own_row = jnp.where(own_row >= Q_BLOCK, own_row - Q_BLOCK, own_row)
    later = lax.broadcasted_iota(jnp.int32, own_row.shape, 1) > own_row
    low_lane = lax.broadcasted_iota(jnp.int32, (1, LANES), 1) < SEL_BLOCK

    def score(j):
        at = pl.ds(pl.multiple_of(j * Q_BLOCK, Q_BLOCK), Q_BLOCK)
        own = j * (Q_BLOCK // SEL_BLOCK)
        parts = [held[own + b] for b in range(Q_BLOCK // SEL_BLOCK)]
        first = me * span + own
        biases = []
        for a in range(FAR_PICKS):
            pick = near_sm[a, me * q_blocks + j]
            usable = pick < first
            owner = jnp.where(usable, pick // span, me)
            parts.append(got[owner, j])
            biases.append(jnp.where(usable, 0.0, MASKED))
        both = jnp.concatenate(parts, axis=0)
        q = jnp.concatenate([qt[0, at], qt[1, at]], axis=0)
        return nt_dot(q, both), both, biases

    def weights(s, biases):
        pieces = [jnp.where(later, MASKED, s[:, :Q_BLOCK])]
        for a in range(0, FAR_PICKS, 2):
            c = Q_BLOCK + a * SEL_BLOCK
            pieces.append(s[:, c : c + LANES] + jnp.where(low_lane, biases[a], biases[a + 1]))
        top = functools.reduce(jnp.maximum, pieces)
        top = jnp.max(top, axis=-1, keepdims=True)
        return [jnp.exp2(p - top).astype(jnp.bfloat16) for p in pieces]

    def settle(j, e, both):
        at = pl.ds(pl.multiple_of(j * Q_BLOCK, Q_BLOCK), Q_BLOCK)
        both = jnp.where(low_lanes(both.shape), jnp.ones_like(both), both)
        o = jnp.dot(jnp.concatenate(e, axis=1), both, preferred_element_type=jnp.float32)
        o = merge(o * pltpu.roll(1.0 / o, HEAD_DIM, 1), Q_BLOCK)
        g = pltpu.roll(pltpu_pad(gate[at]), LANES - 2 * rank, 1)
        mix[at] = (oc[at] + o * gate_lanes(g, 16, o.shape)).astype(jnp.bfloat16)

    def choose(step, carry):
        target = (rank + 1 + step) % RANKS
        js = [target * group + u for u in range(group)]
        scored = [score(j) for j in js]
        es = [weights(s, biases) for s, _, biases in scored]
        for j, e, (_, both, _) in zip(js, es, scored):
            settle(j, e, both)
        pl.when(step > 0)(lambda: mix_copy(step - 1).start())
        return carry

    lax.fori_loop(0, RANKS, choose, 0)

    own_at = pl.ds(pl.multiple_of(rank * rank_rows, rank_rows), rank_rows)
    heard[rank] = mix[own_at]
    for n in range(len(MOVES)):
        copy, _, sends, _ = sum_copy(n, me)
        pl.when(sends)(copy.wait_send)
    for n in range(len(HOPS)):
        copy, _, _, sends, _ = hop(n)
        pl.when(sends)(copy.wait_send)
    for n in range(4):
        copy, sends = span_copy(n)
        pl.when(sends)(copy.wait_send)
    copies[9].wait()
    for step in range(RANKS - 1):
        mix_copy(step).wait_send()
        mix_copy(step).wait_recv()

    lhs = jnp.concatenate([heard[t] for t in range(RANKS)], axis=1)

    def finish(c, carry):
        at = pl.ds(pl.multiple_of(c * 512, 512), 512)
        out_ref[:, at] = jnp.dot(lhs, wo[:, at], preferred_element_type=jnp.float32).astype(jnp.bfloat16)
        return carry

    lax.fori_loop(0, width // 512, finish, 0)


def rope_tables(length):
    half = HEAD_DIM // 2
    inverse = ROPE_BASE ** (-(np.arange(half, dtype=np.float32)) / np.float32(half))
    inverse = np.tile(inverse.astype(np.float32).astype(np.float64), LANES // half)

    def table(positions):
        angle = positions.astype(np.float64)[:, None] * inverse[None, :]
        return np.cos(angle), np.sin(angle)

    low = np.concatenate(table(np.arange(SEL_BLOCK)), axis=0).astype(np.float32)
    high = np.concatenate(table(np.arange(length // SEL_BLOCK) * SEL_BLOCK), axis=1).astype(np.float32)
    return jnp.asarray(low), jnp.asarray(high)


def per_device(
    tokens,
    norm_gain,
    query_weight,
    cmp_key_weight,
    cmp_value_weight,
    sel_key_weight,
    sel_value_weight,
    branch_weight,
    key_embed,
    key_inner,
    key_outer,
    value_embed,
    value_inner,
    value_outer,
    out_weight,
    chosen,
):
    rows, width = tokens.shape
    f32, bf16 = jnp.float32, jnp.bfloat16
    low, high = rope_tables(rows * OWNERS)
    span = rows // SEL_BLOCK
    q_blocks = rows // Q_BLOCK
    blocks = rows // CMP_BLOCK
    rank_rows = rows // RANKS
    picks = chosen.shape[1]
    operands = (
        chosen[0].T,
        norm_gain,
        key_embed[0],
        key_outer[0],
        value_embed[0],
        value_outer[0],
        low,
        high,
        tokens,
        query_weight,
        sel_key_weight.T,
        sel_value_weight.T,
        cmp_key_weight.T,
        cmp_value_weight.T,
        branch_weight.transpose(0, 2, 1).reshape(32, width),
        key_inner[0].T,
        value_inner[0].T,
        out_weight,
    )
    vmem = pl.BlockSpec(memory_space=pltpu.VMEM)
    hbm = pl.BlockSpec(memory_space=pl.ANY)
    dma = pltpu.SemaphoreType.DMA
    moves = len(MOVES)
    return pl.pallas_call(
        layer_kernel,
        in_specs=[vmem] * 7 + [hbm] * 11,
        out_specs=vmem,
        out_shape=pltpu.VMEM((rank_rows, width), bf16),
        scratch_shapes=[
            pltpu.VMEM((span, 2 * LANES), f32),
            pltpu.VMEM((rows, width), bf16),
            pltpu.VMEM((width, LANES), bf16),
            pltpu.VMEM((288, width), bf16),
            pltpu.VMEM((416, width), bf16),
            pltpu.VMEM((HEAD_DIM, width), bf16),
            pltpu.VMEM((HEAD_DIM, width), bf16),
            pltpu.VMEM(out_weight.shape, bf16),
            pltpu.VMEM((span, SEL_BLOCK, LANES), bf16),
            pltpu.VMEM((span, SEL_BLOCK, LANES), bf16),
            pltpu.VMEM((span, SEL_BLOCK, LANES), bf16),
            pltpu.VMEM((len(HOPS), q_blocks, SEL_BLOCK, LANES), bf16),
            pltpu.VMEM((OWNERS, q_blocks, SEL_BLOCK, LANES), bf16),
            pltpu.VMEM((2, rows, LANES), bf16),
            pltpu.VMEM((2, rows, LANES), bf16),
            pltpu.VMEM((rows, LANES), f32),
            pltpu.VMEM((rows, 32), f32),
            pltpu.VMEM((rows, LANES), f32),
            pltpu.VMEM((OWNERS, blocks, LANES), bf16),
            pltpu.VMEM((OWNERS * blocks, LANES), bf16),
            pltpu.VMEM((OWNERS * blocks, LANES), bf16),
            pltpu.VMEM((rows, LANES), f32),
            pltpu.VMEM((rows, LANES), bf16),
            pltpu.VMEM((RANKS, rank_rows, LANES), bf16),
            pltpu.VMEM((2, FAR_PICKS, picks), jnp.int32),
            pltpu.SMEM((FAR_PICKS, picks), jnp.int32),
            pltpu.SMEM((FAR_PICKS, picks), jnp.int32),
            dma((rows // 512,)),
            dma((12,)),
            dma((4,)),
            dma((2,)),
            dma((len(HOPS),)),
            dma((len(HOPS),)),
            dma((moves,)),
            dma((moves,)),
            dma((RANKS,)),
            dma((RANKS,)),
        ],
        compiler_params=pltpu.CompilerParams(
            collective_id=0, has_side_effects=True, vmem_limit_bytes=60 * 1024 * 1024
        ),
        cost_estimate=pl.CostEstimate(flops=int(4e10), bytes_accessed=int(2e7), transcendentals=0),
        name="layer",
    )(*operands)


def solution(mesh):
    placed = (
        P("kv", None),
        P(),
        P(None, "tp"),
        P(None, "tp"),
        P(None, "tp"),
        P(None, "tp"),
        P(None, "tp"),
        P(),
        P("tp", None, None),
        P("tp", None, None),
        P("tp", None, None),
        P("tp", None, None),
        P("tp", None, None),
        P("tp", None, None),
        P(),
        P("tp", None, None),
    )
    return jax.shard_map(
        per_device, mesh=mesh, in_specs=placed, out_specs=P(("kv", "tp"), None), check_vma=False
    )
```

```python
import functools
import math

import jax
import jax.numpy as jnp
import numpy as np
from jax import lax
from jax.experimental import pallas as pl
from jax.experimental.pallas import tpu as pltpu
from jax.sharding import PartitionSpec as P

HEAD_DIM = 64
CMP_BLOCK = 32
SEL_BLOCK = 64
Q_BLOCK = 128
FAR_PICKS = 8
LANES = 2 * HEAD_DIM
PLANES = 4
ACROSS = 4
OWNERS = PLANES * ACROSS
RANKS = 8
MESH = pl.DeviceIdType.MESH

ROPE_BASE = 10000.0
norm_eps = 1e-06
MASKED = -1e30

MOVES = [(dz, dx) for dx in (2, 1, 3, 0) for dz in (2, 1, 3, 0) if (dz, dx) != (0, 0)]
OWN, NEAR, FAR, SKIP = range(4)
LATE = [(FAR, 1), (FAR, 3), (SKIP, 3), (SKIP, 2)]
EARLY_PICKS = FAR_PICKS - len(LATE)
HOPS = [(kind, dx) for kind in (OWN, NEAR, FAR) for dx in (2, 1, 3)] + [(SKIP, dx) for dx in (0, 1, 3, 2)]


def nt_dot(a, b):
    return lax.dot_general(a, b, (((1,), (1,)), ((), ())), preferred_element_type=jnp.float32)


def low_lanes(shape):
    return lax.broadcasted_iota(jnp.int32, shape, 1) < HEAD_DIM


def gate_lanes(gate, first, shape):
    return jnp.where(low_lanes(shape), gate[:, first : first + 1], gate[:, first + 1 : first + 2])


def merge(out, rows):
    low = low_lanes((rows, LANES))
    return jnp.where(low, pltpu.roll(out[:rows], HEAD_DIM, 1), out[rows:])


def layer_kernel(
    chosen_ref,
    gain_ref,
    ke_ref,
    ko_ref,
    ve_ref,
    vo_ref,
    lo_ref,
    hi_hbm,
    tok_hbm,
    wq_hbm,
    wsk_hbm,
    wsv_hbm,
    wck_hbm,
    wcv_hbm,
    wg_hbm,
    ki_hbm,
    vi_hbm,
    wo_hbm,
    out_ref,
    hi,
    tok,
    wq,
    raw,
    wt,
    ki,
    vi,
    wo,
    held,
    near,
    far,
    stage,
    got,
    late,
    first_out,
    first_top,
    qp,
    qt,
    ckv,
    gate,
    scales,
    sums,
    keys,
    values,
    oc,
    mix,
    heard,
    pick_vm,
    pick_sm,
    near_sm,
    tok_sem,
    local_sem,
    span_send,
    span_recv,
    send_sem,
    recv_sem,
    sum_send,
    sum_recv,
    mix_send,
    mix_recv,
):
    me, rank = lax.axis_index("kv"), lax.axis_index("tp")
    z, x = me // ACROSS, me % ACROSS
    rows, width = tok.shape
    tile = 512
    tiles = rows // tile
    q_blocks = rows // Q_BLOCK
    span = rows // SEL_BLOCK
    blocks = rows // CMP_BLOCK
    scale = HEAD_DIM ** (-0.5) * math.log2(math.e)

    sums[...] = jnp.zeros_like(sums)
    barrier = pltpu.get_barrier_semaphore()
    for d in range(1, OWNERS):
        pl.semaphore_signal(barrier, inc=1, device_id={"kv": (me + d) % OWNERS}, device_id_type=MESH)
    for d in range(1, RANKS):
        pl.semaphore_signal(barrier, inc=1, device_id={"tp": (rank + d) % RANKS}, device_id_type=MESH)

    loads = [
        (wq_hbm, wq),
        (wsk_hbm, raw.at[pl.ds(0, 64)]),
        (wsv_hbm, raw.at[pl.ds(64, 64)]),
        (wck_hbm, raw.at[pl.ds(128, 64)]),
        (wcv_hbm, raw.at[pl.ds(192, 64)]),
        (wg_hbm, raw.at[pl.ds(256, 32)]),
        (hi_hbm.at[pl.ds(pl.multiple_of(me * span, span), span)], hi),
        (ki_hbm, ki),
        (vi_hbm, vi),
        (wo_hbm, wo),
    ]
    copies = [pltpu.make_async_copy(a, b, local_sem.at[n]) for n, (a, b) in enumerate(loads)]
    tok_copies = [
        pltpu.make_async_copy(tok_hbm.at[pl.ds(n * tile, tile)], tok.at[pl.ds(n * tile, tile)], tok_sem.at[n])
        for n in range(tiles)
    ]
    for copy in copies[:7]:
        copy.start()
    for copy in tok_copies:
        copy.start()
    for copy in copies[7:]:
        copy.start()

    chosen = chosen_ref[...]
    near_owner, far_owner = jnp.where(z == 0, me + ACROSS, me - ACROSS), x
    line = lax.broadcasted_iota(jnp.int32, chosen.shape, 0)
    index = jnp.zeros(chosen.shape, jnp.int32)
    for kind, owner in ((OWN, me), (NEAR, near_owner), (FAR, far_owner)):
        inside = jnp.where(chosen // span == owner, chosen % span, 0)
        index = jnp.where(line == kind, jnp.sum(inside, axis=0, keepdims=True), index)
    pick_vm[0] = index
    at_block = lax.broadcasted_iota(jnp.int32, chosen.shape, 1) * (Q_BLOCK // SEL_BLOCK)
    usable = chosen < at_block
    owner = chosen // span
    away = lax.rem(x + ACROSS - lax.rem(owner, ACROSS), ACROSS)
    place = jnp.full(chosen.shape, -1, jnp.int32)
    for n, (kind, dx) in enumerate(LATE):
        home, receives = (0, z >= 2) if kind == FAR else (1, z == 3)
        hit = (owner // ACROSS == home) & (away == dx) & usable
        place = jnp.where(hit & receives, n, place)
    code = jnp.where(usable, jnp.where(place >= 0, 32 + place, owner), 64 + me)
    slow = (place >= 0).astype(jnp.int32)
    quick_count = FAR_PICKS - jnp.sum(slow, axis=0, keepdims=True)
    table = jnp.zeros(chosen.shape, jnp.int32)
    before = jnp.zeros((1, chosen.shape[1]), jnp.int32)
    for a in range(FAR_PICKS):
        is_slow = slow[a : a + 1]
        rank_of = jnp.where(is_slow > 0, quick_count + before, a - before)
        table = jnp.where(line == rank_of, code[a : a + 1], table)
        before = before + is_slow
    pick_vm[1] = table
    to_smem = pltpu.make_async_copy(pick_vm.at[0], pick_sm, local_sem.at[len(loads)])
    near_smem = pltpu.make_async_copy(pick_vm.at[1], near_sm, local_sem.at[len(loads) + 1])
    to_smem.start()
    near_smem.start()

    for copy in copies[:7]:
        copy.wait()

    gain = gain_ref[...].astype(jnp.float32).reshape(1, width)
    eye = (
        lax.broadcasted_iota(jnp.int32, (LANES, LANES), 0)
        == lax.broadcasted_iota(jnp.int32, (LANES, LANES), 1)
    ).astype(jnp.bfloat16)

    def weigh(source, first, count, target):
        def one(i, carry):
            r = pl.ds(pl.multiple_of(first + i * 16, 16), 16)
            t = pl.ds(pl.multiple_of(target + i * 16, 16), 16)
            wt[t] = (source[r].astype(jnp.float32) * gain).astype(jnp.bfloat16)
            return carry

        lax.fori_loop(0, count // 16, one, 0)

    weigh(raw, 0, 128, 0)
    for c in range(width // 256):
        cut = slice(c * 256, (c + 1) * 256)
        turned = nt_dot(eye, wq[cut])
        wt[128:256, cut] = (turned * gain[:, cut]).astype(jnp.bfloat16)

    first_half = lax.broadcasted_iota(jnp.int32, (1, LANES), 1) % HEAD_DIM < HEAD_DIM // 2
    flag = (lax.broadcasted_iota(jnp.int32, (1, LANES), 1) == HEAD_DIM).astype(jnp.float32)
    quarter = HEAD_DIM // 2

    def turn(v, cosine, sine):
        swapped = jnp.where(first_half, pltpu.roll(v, LANES - quarter, 1), pltpu.roll(v, quarter, 1))
        return v * cosine + swapped * sine

    def project(i):
        at = pl.ds(i * tile, tile)
        v = tok[at]
        y = nt_dot(v, wt[0:256])
        w = v.astype(jnp.float32)
        inv = lax.rsqrt(jnp.mean(w * w, axis=-1, keepdims=True) + norm_eps)
        scales[at] = jnp.broadcast_to(inv, (tile, LANES))
        y = y * inv
        cos_lo, sin_lo = lo_ref[0:64], lo_ref[64:128]
        for g in range(tile // SEL_BLOCK):
            b = i * (tile // SEL_BLOCK) + g
            cut = slice(g * SEL_BLOCK, (g + 1) * SEL_BLOCK)
            cos_hi, sin_hi = hi[pl.ds(b, 1), 0:LANES], hi[pl.ds(b, 1), LANES : 2 * LANES]
            cosine = cos_hi * cos_lo - sin_hi * sin_lo
            sine = sin_hi * cos_lo + cos_hi * sin_lo
            sine = jnp.where(first_half, -sine, sine)
            part = y[cut, 0:LANES]
            low = low_lanes(part.shape)
            held[b] = jnp.where(low, turn(part, cosine, sine), part).astype(jnp.bfloat16)
            part = y[cut, LANES : 2 * LANES] * scale
            to = pl.ds(b * SEL_BLOCK, SEL_BLOCK)
            for ref, q, rest in ((qp, part, flag), (qt, turn(part, cosine, sine), 0.0)):
                ref[0, to] = jnp.where(low, q, rest).astype(jnp.bfloat16)
                ref[1, to] = jnp.where(low, pltpu.roll(q, HEAD_DIM, 1), rest).astype(jnp.bfloat16)

    def route(dz, dx):
        there = ((z + dz) % PLANES) * ACROSS + (x + dx) % ACROSS
        here = ((z - dz) % PLANES) * ACROSS + (x - dx) % ACROSS
        if dz == 0:
            return there, x + dx < ACROSS, here, x >= dx
        return there, z + dz < PLANES, here, z >= dz

    def span_copy(n, c):
        step, sends, source, target = (
            (1, z < 3, held, near),
            (3, z == 1, held, near),
            (3, z == 0, held, far),
            (3, z == 3, far, far),
        )[n]
        at = pl.ds(c * (span // tiles), span // tiles)
        return (
            pltpu.make_async_remote_copy(
                src_ref=source.at[at],
                dst_ref=target.at[at],
                send_sem=span_send.at[n, c],
                recv_sem=span_recv.at[n // 2, c],
                device_id={"kv": lax.rem(me + step * ACROSS, OWNERS)},
                device_id_type=MESH,
            ),
            sends,
        )

    for i in range(tiles):
        tok_copies[i].wait()
        project(i)
        if i == 0:
            pl.semaphore_wait(barrier, OWNERS + RANKS - 2)
        for n in range(3):
            copy, sends = span_copy(n, i)
            pl.when(sends)(copy.start)

    to_smem.wait()
    near_smem.wait()

    def hop(n):
        kind, dx = HOPS[n]
        column = lax.rem(x + dx, ACROSS)
        back = lax.rem(x + ACROSS - dx, ACROSS)
        if kind == OWN:
            owner, source, sends, gets = me, held, x + dx < ACROSS, x >= dx
        elif kind == NEAR:
            owner, source, sends, gets = near_owner, near, z >= 1, z >= 1
        elif kind == FAR:
            owner, source, sends, gets = far_owner, far, z >= 2, z >= 2
        else:
            owner, source, sends, gets = near_owner, near, z == 0, z == 3
        there = (3 if kind == SKIP else z) * ACROSS + column
        copy = pltpu.make_async_remote_copy(
            src_ref=stage.at[n],
            dst_ref=late.at[LATE.index(HOPS[n])] if HOPS[n] in LATE else got.at[owner],
            send_sem=send_sem.at[n],
            recv_sem=recv_sem.at[n],
            device_id={"kv": there},
            device_id_type=MESH,
        )
        return copy, there, source, sends, gets

    def gather(source, kind, target, first):
        def one(j, carry):
            target[j] = source[pick_sm[kind, first + j]]
            return carry

        lax.fori_loop(0, q_blocks, one, 0)

    def send_hops(*kinds):
        for n, (kind, dx) in enumerate(HOPS):
            if kind in kinds:
                copy, there, source, sends, _ = hop(n)

                def go(n=n, kind=kind, copy=copy, there=there, source=source):
                    gather(source, NEAR if kind == SKIP else kind, stage.at[n], there * q_blocks)
                    copy.start()

                pl.when(sends)(go)

    send_hops(OWN)

    weigh(raw, 128, 160, 256)

    def project_more(i):
        at = pl.ds(i * tile, tile)
        y = nt_dot(tok[at], wt[256:416])
        inv = scales[at]
        ckv[at] = (y[:, 0:LANES] * inv).astype(jnp.bfloat16).astype(jnp.float32)
        gate[at] = jax.nn.sigmoid(y[:, LANES : LANES + 32] * inv[:, 0:32])

    def hand_back(c):
        span_copy(2, c)[0].wait_recv()
        span_copy(3, c)[0].start()

    for c in range(tiles):
        project_more(c)
        pl.when(z == 3)(functools.partial(hand_back, c))
    for copy in copies[7:9]:
        copy.wait()

    low = low_lanes((blocks, LANES))

    def summarize(is_value, e_ref, i_ref, o_ref):
        parts = []
        embed = e_ref[...].astype(jnp.float32)
        for c in range(0, CMP_BLOCK, 2):
            a = ckv[pl.ds(c, blocks, stride=CMP_BLOCK), :]
            b = ckv[pl.ds(c + 1, blocks, stride=CMP_BLOCK), :]
            if is_value:
                pair = jnp.where(low, pltpu.roll(a, HEAD_DIM, 1), b)
            else:
                pair = jnp.where(low, a, pltpu.roll(b, HEAD_DIM, 1))
            e = jnp.concatenate([embed[c : c + 1], embed[c + 1 : c + 2]], axis=1)
            parts.append((pair + e).astype(jnp.bfloat16))
        flat = jnp.concatenate(parts, axis=1)
        hidden = jax.nn.gelu(nt_dot(flat, i_ref[...])).astype(jnp.bfloat16)
        return jnp.dot(hidden, o_ref[...], preferred_element_type=jnp.float32)

    sk = summarize(False, ke_ref, ki, ko_ref)
    sv = summarize(True, ve_ref, vi, vo_ref)
    sums[me] = jnp.concatenate([sk, sv], axis=1).astype(jnp.bfloat16)

    def sum_copy(n, owner):
        there, sends, here, gets = route(*MOVES[n])
        copy = pltpu.make_async_remote_copy(
            src_ref=sums.at[owner],
            dst_ref=sums.at[owner],
            send_sem=sum_send.at[n],
            recv_sem=sum_recv.at[n],
            device_id={"kv": there},
            device_id_type=MESH,
        )
        return copy, here, sends, gets

    for n in range(len(MOVES)):
        copy, _, sends, _ = sum_copy(n, me)
        pl.when(sends)(copy.start)
    gather(held, OWN, got.at[me], me * q_blocks)

    def pass_near():
        send_hops(NEAR)
        gather(near, NEAR, got.at[near_owner], me * q_blocks)

    def pass_far():
        for c in range(tiles):
            pl.when(z == 2)(span_copy(2, c)[0].wait_recv)
        send_hops(FAR)
        gather(far, FAR, got.at[far_owner], me * q_blocks)

    for c in range(tiles):
        span_copy(0, c)[0].wait_recv()
    send_hops(SKIP)
    pl.when(z >= 1)(pass_near)
    pl.when(z >= 2)(pass_far)
    for n in range(len(MOVES)):
        _, here, _, gets = sum_copy(n, me)
        copy, _, _, _ = sum_copy(n, here)
        pl.when(gets)(copy.wait_recv)

    lane = lax.broadcasted_iota(jnp.int32, (blocks, LANES), 1)
    for d in range(OWNERS):
        owner = lax.rem(me + d, OWNERS)
        both = sums[owner]
        bar = jnp.where(owner > me, MASKED, 0.0).astype(jnp.bfloat16)
        rows_at = slice(d * blocks, (d + 1) * blocks)
        keys[rows_at] = jnp.where(lane == HEAD_DIM, bar, both)
        values[rows_at] = jnp.where(lane < HEAD_DIM, jnp.ones_like(both), both)

    part = 256

    def compress(i, carry):
        at = pl.ds(pl.multiple_of(i * part, part), part)
        pos = i * part + lax.broadcasted_iota(jnp.int32, (part, 1), 0)
        lane = lax.broadcasted_iota(jnp.int32, (1, LANES), 1)
        scored = [nt_dot(qp[h, at], keys[...]) for h in range(2)]
        outs = []
        for s in scored:
            own = jnp.where((lane >= blocks) | ((lane + 1) * CMP_BLOCK - 1 <= pos), s[:, :LANES], MASKED)
            pieces = [own] + [s[:, c : c + LANES] for c in range(LANES, OWNERS * blocks, LANES)]
            top = jnp.max(functools.reduce(jnp.maximum, pieces), axis=-1, keepdims=True)
            e = jnp.concatenate([jnp.exp2(p - top).astype(jnp.bfloat16) for p in pieces], axis=1)
            o = jnp.dot(e, values[...], preferred_element_type=jnp.float32)
            outs.append(o * pltpu.roll(1.0 / o, HEAD_DIM, 1))
        o = jnp.where(low_lanes(outs[0].shape), pltpu.roll(outs[0], HEAD_DIM, 1), outs[1])
        o = jnp.where(me * rows + pos >= CMP_BLOCK - 1, o, 0.0)
        g = pltpu.roll(pltpu_pad(gate[at]), LANES - 2 * rank, 1)
        oc[at] = o * gate_lanes(g, 0, o.shape)
        return carry

    def pltpu_pad(g):
        return jnp.concatenate([g, g, g, g], axis=1)

    lax.fori_loop(0, rows // part, compress, 0)

    rank_rows = rows // RANKS
    group = rank_rows // Q_BLOCK

    def mix_target(step):
        mask = RANKS - 1 - step
        return sum((rank // w + mask // w) % 2 * w for w in (4, 2, 1))

    def mix_copy(step):
        target = mix_target(step)
        at = pl.ds(pl.multiple_of(target * rank_rows, rank_rows), rank_rows)
        return pltpu.make_async_remote_copy(
            src_ref=mix.at[at],
            dst_ref=heard.at[rank],
            send_sem=mix_send.at[step],
            recv_sem=mix_recv.at[step],
            device_id={"tp": target},
            device_id_type=MESH,
        )

    own_row = lax.broadcasted_iota(jnp.int32, (2 * Q_BLOCK, Q_BLOCK), 0)
    own_row = jnp.where(own_row >= Q_BLOCK, own_row - Q_BLOCK, own_row)
    later = lax.broadcasted_iota(jnp.int32, own_row.shape, 1) > own_row
    low_lane = lax.broadcasted_iota(jnp.int32, (1, LANES), 1) < SEL_BLOCK

    def arrive(is_late):
        for n, key in enumerate(HOPS):
            if (key in LATE) == is_late:
                copy, _, _, _, gets = hop(n)
                pl.when(gets)(copy.wait_recv)

    def queries(j):
        at = pl.ds(pl.multiple_of(j * Q_BLOCK, Q_BLOCK), Q_BLOCK)
        return jnp.concatenate([qt[0, at], qt[1, at]], axis=0)

    def with_ones(both):
        return jnp.where(low_lanes(both.shape), jnp.ones_like(both), both)

    def bias_of(a, j):
        return jnp.where(near_sm[a, me * q_blocks + j] < 64, 0.0, MASKED)

    def first_blocks(j):
        own = j * (Q_BLOCK // SEL_BLOCK)
        parts = [held[own + b] for b in range(Q_BLOCK // SEL_BLOCK)]
        for a in range(EARLY_PICKS):
            parts.append(got[near_sm[a, me * q_blocks + j] % OWNERS, j])
        return jnp.concatenate(parts, axis=0)

    def last_blocks(j):
        parts = []
        for a in range(EARLY_PICKS, FAR_PICKS):
            mark = near_sm[a, me * q_blocks + j]
            slow = (mark >= 32) & (mark < 64)
            quick_block = got[jnp.where(slow, me, mark % OWNERS), j]
            slow_block = late[jnp.where(slow, mark - 32, 0), j]
            parts.append(jnp.where(slow, slow_block, quick_block))
        return jnp.concatenate(parts, axis=0)

    def biased(s, j, first):
        return [
            s[:, c : c + LANES]
            + jnp.where(low_lane, bias_of(first + c // SEL_BLOCK, j), bias_of(first + c // SEL_BLOCK + 1, j))
            for c in range(0, s.shape[1], LANES)
        ]

    def start_choice(i, carry):
        js = [i * 2 + u for u in range(2)]
        boths = [first_blocks(j) for j in js]
        scores = [nt_dot(queries(j), both) for j, both in zip(js, boths)]
        done = []
        for j, s in zip(js, scores):
            pieces = [jnp.where(later, MASKED, s[:, :Q_BLOCK])] + biased(s[:, Q_BLOCK:], j, 0)
            top = jnp.max(functools.reduce(jnp.maximum, pieces), axis=-1, keepdims=True)
            done.append((top, jnp.concatenate([jnp.exp2(p - top).astype(jnp.bfloat16) for p in pieces], axis=1)))
        for j, (top, e), both in zip(js, done, boths):
            first_out[j] = jnp.dot(e, with_ones(both), preferred_element_type=jnp.float32)
            first_top[j] = jnp.broadcast_to(top, (2 * Q_BLOCK, LANES))
        return carry

    arrive(False)
    lax.fori_loop(0, q_blocks // 2, start_choice, 0)
    arrive(True)

    def choose(step, carry):
        pl.when(step > 0)(lambda: mix_copy(step - 1).start())
        target = mix_target(step)
        js = [target * group + u for u in range(group)]
        boths = [last_blocks(j) for j in js]
        scores = [nt_dot(queries(j), both) for j, both in zip(js, boths)]
        done = []
        for j, s in zip(js, scores):
            pieces = biased(s, j, EARLY_PICKS)
            old = first_top[j]
            top = jnp.max(functools.reduce(jnp.maximum, pieces), axis=-1, keepdims=True)
            top = jnp.maximum(old, top)
            e = jnp.concatenate([jnp.exp2(p - top).astype(jnp.bfloat16) for p in pieces], axis=1)
            done.append((e, jnp.exp2(old - top)))
        for j, (e, keep), both in zip(js, done, boths):
            at = pl.ds(pl.multiple_of(j * Q_BLOCK, Q_BLOCK), Q_BLOCK)
            o = first_out[j] * keep + jnp.dot(e, with_ones(both), preferred_element_type=jnp.float32)
            o = merge(o * pltpu.roll(1.0 / o, HEAD_DIM, 1), Q_BLOCK)
            g = pltpu.roll(pltpu_pad(gate[at]), LANES - 2 * rank, 1)
            mix[at] = (oc[at] + o * gate_lanes(g, 16, o.shape)).astype(jnp.bfloat16)
        return carry

    lax.fori_loop(0, RANKS, choose, 0)

    own_at = pl.ds(pl.multiple_of(rank * rank_rows, rank_rows), rank_rows)
    heard[rank] = mix[own_at]
    for n in range(len(MOVES)):
        copy, _, sends, _ = sum_copy(n, me)
        pl.when(sends)(copy.wait_send)
    for n in range(len(HOPS)):
        copy, _, _, sends, _ = hop(n)
        pl.when(sends)(copy.wait_send)
    for n in range(4):
        for c in range(tiles):
            copy, sends = span_copy(n, c)
            pl.when(sends)(copy.wait_send)
    copies[9].wait()
    for step in range(RANKS - 1):
        mix_copy(step).wait_send()
        mix_copy(step).wait_recv()

    lhs = jnp.concatenate([heard[t] for t in range(RANKS)], axis=1)

    def finish(c, carry):
        at = pl.ds(pl.multiple_of(c * 512, 512), 512)
        out_ref[:, at] = jnp.dot(lhs, wo[:, at], preferred_element_type=jnp.float32).astype(jnp.bfloat16)
        return carry

    lax.fori_loop(0, width // 512, finish, 0)


def rope_tables(length):
    half = HEAD_DIM // 2
    inverse = ROPE_BASE ** (-(np.arange(half, dtype=np.float32)) / np.float32(half))
    inverse = np.tile(inverse.astype(np.float32).astype(np.float64), LANES // half)

    def table(positions):
        angle = positions.astype(np.float64)[:, None] * inverse[None, :]
        return np.cos(angle), np.sin(angle)

    low = np.concatenate(table(np.arange(SEL_BLOCK)), axis=0).astype(np.float32)
    high = np.concatenate(table(np.arange(length // SEL_BLOCK) * SEL_BLOCK), axis=1).astype(np.float32)
    return jnp.asarray(low), jnp.asarray(high)


def per_device(
    tokens,
    norm_gain,
    query_weight,
    cmp_key_weight,
    cmp_value_weight,
    sel_key_weight,
    sel_value_weight,
    branch_weight,
    key_embed,
    key_inner,
    key_outer,
    value_embed,
    value_inner,
    value_outer,
    out_weight,
    chosen,
):
    rows, width = tokens.shape
    f32, bf16 = jnp.float32, jnp.bfloat16
    low, high = rope_tables(rows * OWNERS)
    span = rows // SEL_BLOCK
    q_blocks = rows // Q_BLOCK
    blocks = rows // CMP_BLOCK
    rank_rows = rows // RANKS
    picks = chosen.shape[1]
    operands = (
        chosen[0].T,
        norm_gain,
        key_embed[0],
        key_outer[0],
        value_embed[0],
        value_outer[0],
        low,
        high,
        tokens,
        query_weight,
        sel_key_weight.T,
        sel_value_weight.T,
        cmp_key_weight.T,
        cmp_value_weight.T,
        branch_weight.transpose(0, 2, 1).reshape(32, width),
        key_inner[0].T,
        value_inner[0].T,
        out_weight,
    )
    vmem = pl.BlockSpec(memory_space=pltpu.VMEM)
    hbm = pl.BlockSpec(memory_space=pl.ANY)
    dma = pltpu.SemaphoreType.DMA
    moves = len(MOVES)
    return pl.pallas_call(
        layer_kernel,
        in_specs=[vmem] * 7 + [hbm] * 11,
        out_specs=vmem,
        out_shape=pltpu.VMEM((rank_rows, width), bf16),
        scratch_shapes=[
            pltpu.VMEM((span, 2 * LANES), f32),
            pltpu.VMEM((rows, width), bf16),
            pltpu.VMEM((width, LANES), bf16),
            pltpu.VMEM((288, width), bf16),
            pltpu.VMEM((416, width), bf16),
            pltpu.VMEM((HEAD_DIM, width), bf16),
            pltpu.VMEM((HEAD_DIM, width), bf16),
            pltpu.VMEM(out_weight.shape, bf16),
            pltpu.VMEM((span, SEL_BLOCK, LANES), bf16),
            pltpu.VMEM((span, SEL_BLOCK, LANES), bf16),
            pltpu.VMEM((span, SEL_BLOCK, LANES), bf16),
            pltpu.VMEM((len(HOPS), q_blocks, SEL_BLOCK, LANES), bf16),
            pltpu.VMEM((OWNERS, q_blocks, SEL_BLOCK, LANES), bf16),
            pltpu.VMEM((len(LATE), q_blocks, SEL_BLOCK, LANES), bf16),
            pltpu.VMEM((q_blocks, 2 * Q_BLOCK, LANES), f32),
            pltpu.VMEM((q_blocks, 2 * Q_BLOCK, LANES), f32),
            pltpu.VMEM((2, rows, LANES), bf16),
            pltpu.VMEM((2, rows, LANES), bf16),
            pltpu.VMEM((rows, LANES), f32),
            pltpu.VMEM((rows, 32), f32),
            pltpu.VMEM((rows, LANES), f32),
            pltpu.VMEM((OWNERS, blocks, LANES), bf16),
            pltpu.VMEM((OWNERS * blocks, LANES), bf16),
            pltpu.VMEM((OWNERS * blocks, LANES), bf16),
            pltpu.VMEM((rows, LANES), f32),
            pltpu.VMEM((rows, LANES), bf16),
            pltpu.VMEM((RANKS, rank_rows, LANES), bf16),
            pltpu.VMEM((2, FAR_PICKS, picks), jnp.int32),
            pltpu.SMEM((FAR_PICKS, picks), jnp.int32),
            pltpu.SMEM((FAR_PICKS, picks), jnp.int32),
            dma((rows // 512,)),
            dma((12,)),
            dma((4, 4)),
            dma((2, 4)),
            dma((len(HOPS),)),
            dma((len(HOPS),)),
            dma((moves,)),
            dma((moves,)),
            dma((RANKS,)),
            dma((RANKS,)),
        ],
        compiler_params=pltpu.CompilerParams(
            collective_id=0, has_side_effects=True, vmem_limit_bytes=60 * 1024 * 1024
        ),
        cost_estimate=pl.CostEstimate(flops=int(4e10), bytes_accessed=int(2e7), transcendentals=0),
        name="layer",
    )(*operands)


def solution(mesh):
    placed = (
        P("kv", None),
        P(),
        P(None, "tp"),
        P(None, "tp"),
        P(None, "tp"),
        P(None, "tp"),
        P(None, "tp"),
        P(),
        P("tp", None, None),
        P("tp", None, None),
        P("tp", None, None),
        P("tp", None, None),
        P("tp", None, None),
        P("tp", None, None),
        P(),
        P("tp", None, None),
    )
    return jax.shard_map(
        per_device, mesh=mesh, in_specs=placed, out_specs=P(("kv", "tp"), None), check_vma=False
    )
```

```python
import functools
import math

import jax
import jax.numpy as jnp
import numpy as np
from jax import lax
from jax.experimental import pallas as pl
from jax.experimental.pallas import tpu as pltpu
from jax.sharding import PartitionSpec as P

HEAD_DIM = 64
CMP_BLOCK = 32
SEL_BLOCK = 64
Q_BLOCK = 128
FAR_PICKS = 8
LANES = 2 * HEAD_DIM
PLANES = 4
ACROSS = 4
OWNERS = PLANES * ACROSS
RANKS = 8
MESH = pl.DeviceIdType.MESH

ROPE_BASE = 10000.0
norm_eps = 1e-06
MASKED = -1e30

MOVES = [(dz, dx) for dx in (2, 1, 3, 0) for dz in (2, 1, 3, 0) if (dz, dx) != (0, 0)]
OWN, NEAR, FAR, SKIP = range(4)
HALVES = 2
HOPS = [(OWN, dx, half) for half in range(HALVES) for dx in (2, 1, 3)]
for half in range(HALVES):
    HOPS += [(SKIP, dx, half) for dx in (0, 1, 3, 2)]
    HOPS += [(kind, dx, half) for kind in (NEAR, FAR) for dx in (2, 1, 3)]


def nt_dot(a, b):
    return lax.dot_general(a, b, (((1,), (1,)), ((), ())), preferred_element_type=jnp.float32)


def low_lanes(shape):
    return lax.broadcasted_iota(jnp.int32, shape, 1) < HEAD_DIM


def gate_lanes(gate, first, shape):
    return jnp.where(low_lanes(shape), gate[:, first : first + 1], gate[:, first + 1 : first + 2])


def merge(out, rows):
    low = low_lanes((rows, LANES))
    return jnp.where(low, pltpu.roll(out[:rows], HEAD_DIM, 1), out[rows:])


def layer_kernel(
    chosen_ref,
    gain_ref,
    ke_ref,
    ko_ref,
    ve_ref,
    vo_ref,
    lo_ref,
    hi_hbm,
    tok_hbm,
    wq_hbm,
    wsk_hbm,
    wsv_hbm,
    wck_hbm,
    wcv_hbm,
    wg_hbm,
    ki_hbm,
    vi_hbm,
    wo_hbm,
    out_ref,
    hi,
    tok,
    wq,
    raw,
    wt,
    ki,
    vi,
    wo,
    held,
    near,
    far,
    stage,
    got_even,
    got_odd,
    qp,
    qt,
    ckv,
    gate,
    scales,
    sums,
    keys,
    values,
    oc,
    mix,
    heard,
    pick_vm,
    pick_sm,
    owner_sm,
    tok_sem,
    local_sem,
    span_send,
    span_recv,
    send_sem,
    recv_sem,
    sum_send,
    sum_recv,
    mix_send,
    mix_recv,
):
    me, rank = lax.axis_index("kv"), lax.axis_index("tp")
    z, x = me // ACROSS, me % ACROSS
    rows, width = tok.shape
    tile = 512
    tiles = rows // tile
    q_blocks = rows // Q_BLOCK
    span = rows // SEL_BLOCK
    blocks = rows // CMP_BLOCK
    got = (got_even, got_odd)
    scale = HEAD_DIM ** (-0.5) * math.log2(math.e)

    sums[...] = jnp.zeros_like(sums)
    barrier = pltpu.get_barrier_semaphore()
    for d in range(1, OWNERS):
        pl.semaphore_signal(barrier, inc=1, device_id={"kv": (me + d) % OWNERS}, device_id_type=MESH)
    for d in range(1, RANKS):
        pl.semaphore_signal(barrier, inc=1, device_id={"tp": (rank + d) % RANKS}, device_id_type=MESH)

    loads = [
        (wq_hbm, wq),
        (wsk_hbm, raw.at[pl.ds(0, 64)]),
        (wsv_hbm, raw.at[pl.ds(64, 64)]),
        (wck_hbm, raw.at[pl.ds(128, 64)]),
        (wcv_hbm, raw.at[pl.ds(192, 64)]),
        (wg_hbm, raw.at[pl.ds(256, 32)]),
        (hi_hbm.at[pl.ds(pl.multiple_of(me * span, span), span)], hi),
        (ki_hbm, ki),
        (vi_hbm, vi),
        (wo_hbm, wo),
    ]
    copies = [pltpu.make_async_copy(a, b, local_sem.at[n]) for n, (a, b) in enumerate(loads)]
    tok_copies = [
        pltpu.make_async_copy(tok_hbm.at[pl.ds(n * tile, tile)], tok.at[pl.ds(n * tile, tile)], tok_sem.at[n])
        for n in range(tiles)
    ]
    for copy in copies[:7]:
        copy.start()
    for copy in tok_copies:
        copy.start()
    for copy in copies[7:]:
        copy.start()

    chosen = chosen_ref[...]
    near_owner, far_owner = jnp.where(z == 0, me + ACROSS, me - ACROSS), x
    line = lax.broadcasted_iota(jnp.int32, chosen.shape, 0)
    index = jnp.zeros(chosen.shape, jnp.int32)
    for kind, owner in ((OWN, me), (NEAR, near_owner), (FAR, far_owner)):
        inside = jnp.where(chosen // span == owner, chosen % span, 0)
        index = jnp.where(line == kind, jnp.sum(inside, axis=0, keepdims=True), index)
    pick_vm[0] = index
    at_block = lax.broadcasted_iota(jnp.int32, chosen.shape, 1) * (Q_BLOCK // SEL_BLOCK)
    pick_vm[1] = jnp.where(chosen < at_block, chosen // span, 64 + me)
    to_smem = pltpu.make_async_copy(pick_vm.at[0], pick_sm, local_sem.at[len(loads)])
    owner_smem = pltpu.make_async_copy(pick_vm.at[1], owner_sm, local_sem.at[len(loads) + 1])
    to_smem.start()
    owner_smem.start()

    for copy in copies[:7]:
        copy.wait()

    gain = gain_ref[...].astype(jnp.float32).reshape(1, width)
    eye = (
        lax.broadcasted_iota(jnp.int32, (LANES, LANES), 0)
        == lax.broadcasted_iota(jnp.int32, (LANES, LANES), 1)
    ).astype(jnp.bfloat16)

    def weigh(source, first, count, target):
        def one(i, carry):
            r = pl.ds(pl.multiple_of(first + i * 16, 16), 16)
            t = pl.ds(pl.multiple_of(target + i * 16, 16), 16)
            wt[t] = (source[r].astype(jnp.float32) * gain).astype(jnp.bfloat16)
            return carry

        lax.fori_loop(0, count // 16, one, 0)

    weigh(raw, 0, 128, 0)
    for c in range(width // 256):
        cut = slice(c * 256, (c + 1) * 256)
        turned = nt_dot(eye, wq[cut])
        wt[128:256, cut] = (turned * gain[:, cut]).astype(jnp.bfloat16)

    first_half = lax.broadcasted_iota(jnp.int32, (1, LANES), 1) % HEAD_DIM < HEAD_DIM // 2
    flag = (lax.broadcasted_iota(jnp.int32, (1, LANES), 1) == HEAD_DIM).astype(jnp.float32)
    quarter = HEAD_DIM // 2

    def turn(v, cosine, sine):
        swapped = jnp.where(first_half, pltpu.roll(v, LANES - quarter, 1), pltpu.roll(v, quarter, 1))
        return v * cosine + swapped * sine

    def project(i):
        at = pl.ds(i * tile, tile)
        v = tok[at]
        y = nt_dot(v, wt[0:256])
        w = v.astype(jnp.float32)
        inv = lax.rsqrt(jnp.mean(w * w, axis=-1, keepdims=True) + norm_eps)
        scales[at] = jnp.broadcast_to(inv, (tile, LANES))
        y = y * inv
        cos_lo, sin_lo = lo_ref[0:64], lo_ref[64:128]
        for g in range(tile // SEL_BLOCK):
            b = i * (tile // SEL_BLOCK) + g
            cut = slice(g * SEL_BLOCK, (g + 1) * SEL_BLOCK)
            cos_hi, sin_hi = hi[pl.ds(b, 1), 0:LANES], hi[pl.ds(b, 1), LANES : 2 * LANES]
            cosine = cos_hi * cos_lo - sin_hi * sin_lo
            sine = sin_hi * cos_lo + cos_hi * sin_lo
            sine = jnp.where(first_half, -sine, sine)
            part = y[cut, 0:LANES]
            low = low_lanes(part.shape)
            held[b] = jnp.where(low, turn(part, cosine, sine), part).astype(jnp.bfloat16)
            part = y[cut, LANES : 2 * LANES] * scale
            to = pl.ds(b * SEL_BLOCK, SEL_BLOCK)
            for ref, q, rest in ((qp, part, flag), (qt, turn(part, cosine, sine), 0.0)):
                ref[0, to] = jnp.where(low, q, rest).astype(jnp.bfloat16)
                ref[1, to] = jnp.where(low, pltpu.roll(q, HEAD_DIM, 1), rest).astype(jnp.bfloat16)

    def route(dz, dx):
        there = ((z + dz) % PLANES) * ACROSS + (x + dx) % ACROSS
        here = ((z - dz) % PLANES) * ACROSS + (x - dx) % ACROSS
        if dz == 0:
            return there, x + dx < ACROSS, here, x >= dx
        return there, z + dz < PLANES, here, z >= dz

    def span_copy(n, c):
        step, sends, source, target = (
            (1, z < 3, held, near),
            (3, z == 1, held, near),
            (3, z == 0, held, far),
            (3, z == 3, far, far),
        )[n]
        at = pl.ds(c * (span // tiles), span // tiles)
        return (
            pltpu.make_async_remote_copy(
                src_ref=source.at[at],
                dst_ref=target.at[at],
                send_sem=span_send.at[n, c],
                recv_sem=span_recv.at[n // 2, c],
                device_id={"kv": lax.rem(me + step * ACROSS, OWNERS)},
                device_id_type=MESH,
            ),
            sends,
        )

    for i in range(tiles):
        tok_copies[i].wait()
        project(i)
        if i == 0:
            pl.semaphore_wait(barrier, OWNERS + RANKS - 2)
        for n in range(3):
            copy, sends = span_copy(n, i)
            pl.when(sends)(copy.start)

    to_smem.wait()
    owner_smem.wait()

    def hop(n):
        kind, dx, half = HOPS[n]
        column = lax.rem(x + dx, ACROSS)
        back = lax.rem(x + ACROSS - dx, ACROSS)
        if kind == OWN:
            owner, source, sends, gets = me, held, x + dx < ACROSS, x >= dx
        elif kind == NEAR:
            owner, source, sends, gets = near_owner, near, z >= 1, z >= 1
        elif kind == FAR:
            owner, source, sends, gets = far_owner, far, z >= 2, z >= 2
        else:
            owner, source, sends, gets = near_owner, near, z == 0, z == 3
        there = (3 if kind == SKIP else z) * ACROSS + column
        copy = pltpu.make_async_remote_copy(
            src_ref=stage.at[n],
            dst_ref=got[half].at[owner],
            send_sem=send_sem.at[n],
            recv_sem=recv_sem.at[n],
            device_id={"kv": there},
            device_id_type=MESH,
        )
        return copy, there, source, sends, gets

    def gather(source, kind, target, first):
        def one(p, carry):
            target[p] = source[pick_sm[kind, first + HALVES * p]]
            return carry

        lax.fori_loop(0, q_blocks // HALVES, one, 0)

    def gather_own(source, kind, owner):
        for half in range(HALVES):
            gather(source, kind, got[half].at[owner], me * q_blocks + half)

    def send_hops(which, part):
        for n, (kind, dx, half) in enumerate(HOPS):
            if kind == which and half == part:
                copy, there, source, sends, _ = hop(n)

                def go(n=n, kind=kind, copy=copy, there=there, source=source):
                    first = there * q_blocks + part
                    gather(source, NEAR if kind == SKIP else kind, stage.at[n], first)
                    copy.start()

                pl.when(sends)(go)

    for half in range(HALVES):
        send_hops(OWN, half)

    weigh(raw, 128, 160, 256)

    def project_more(i):
        at = pl.ds(i * tile, tile)
        y = nt_dot(tok[at], wt[256:416])
        inv = scales[at]
        ckv[at] = (y[:, 0:LANES] * inv).astype(jnp.bfloat16).astype(jnp.float32)
        gate[at] = jax.nn.sigmoid(y[:, LANES : LANES + 32] * inv[:, 0:32])

    def hand_back(c):
        span_copy(2, c)[0].wait_recv()
        span_copy(3, c)[0].start()

    for c in range(tiles):
        project_more(c)
        pl.when(z == 3)(functools.partial(hand_back, c))
    for copy in copies[7:9]:
        copy.wait()

    low = low_lanes((blocks, LANES))

    def summarize(is_value, e_ref, i_ref, o_ref):
        parts = []
        embed = e_ref[...].astype(jnp.float32)
        for c in range(0, CMP_BLOCK, 2):
            a = ckv[pl.ds(c, blocks, stride=CMP_BLOCK), :]
            b = ckv[pl.ds(c + 1, blocks, stride=CMP_BLOCK), :]
            if is_value:
                pair = jnp.where(low, pltpu.roll(a, HEAD_DIM, 1), b)
            else:
                pair = jnp.where(low, a, pltpu.roll(b, HEAD_DIM, 1))
            e = jnp.concatenate([embed[c : c + 1], embed[c + 1 : c + 2]], axis=1)
            parts.append((pair + e).astype(jnp.bfloat16))
        flat = jnp.concatenate(parts, axis=1)
        hidden = jax.nn.gelu(nt_dot(flat, i_ref[...])).astype(jnp.bfloat16)
        return jnp.dot(hidden, o_ref[...], preferred_element_type=jnp.float32)

    sk = summarize(False, ke_ref, ki, ko_ref)
    sv = summarize(True, ve_ref, vi, vo_ref)
    sums[me] = jnp.concatenate([sk, sv], axis=1).astype(jnp.bfloat16)

    def sum_copy(n, owner):
        there, sends, here, gets = route(*MOVES[n])
        copy = pltpu.make_async_remote_copy(
            src_ref=sums.at[owner],
            dst_ref=sums.at[owner],
            send_sem=sum_send.at[n],
            recv_sem=sum_recv.at[n],
            device_id={"kv": there},
            device_id_type=MESH,
        )
        return copy, here, sends, gets

    for n in range(len(MOVES)):
        copy, _, sends, _ = sum_copy(n, me)
        pl.when(sends)(copy.start)
    gather_own(held, OWN, me)
    for c in range(tiles):
        span_copy(0, c)[0].wait_recv()
    for half in range(HALVES):
        send_hops(SKIP, half)
        send_hops(NEAR, half)
        if half == 0:
            for c in range(tiles):
                pl.when(z == 2)(span_copy(2, c)[0].wait_recv)
        send_hops(FAR, half)
    pl.when(z >= 1)(lambda: gather_own(near, NEAR, near_owner))
    pl.when(z >= 2)(lambda: gather_own(far, FAR, far_owner))
    for n in range(len(MOVES)):
        _, here, _, gets = sum_copy(n, me)
        copy, _, _, _ = sum_copy(n, here)
        pl.when(gets)(copy.wait_recv)

    lane = lax.broadcasted_iota(jnp.int32, (blocks, LANES), 1)
    for d in range(OWNERS):
        owner = lax.rem(me + d, OWNERS)
        both = sums[owner]
        bar = jnp.where(owner > me, MASKED, 0.0).astype(jnp.bfloat16)
        rows_at = slice(d * blocks, (d + 1) * blocks)
        keys[rows_at] = jnp.where(lane == HEAD_DIM, bar, both)
        values[rows_at] = jnp.where(lane < HEAD_DIM, jnp.ones_like(both), both)

    part = 256

    def compress(i, carry):
        at = pl.ds(pl.multiple_of(i * part, part), part)
        pos = i * part + lax.broadcasted_iota(jnp.int32, (part, 1), 0)
        lane = lax.broadcasted_iota(jnp.int32, (1, LANES), 1)
        scored = [nt_dot(qp[h, at], keys[...]) for h in range(2)]
        outs = []
        for s in scored:
            own = jnp.where((lane >= blocks) | ((lane + 1) * CMP_BLOCK - 1 <= pos), s[:, :LANES], MASKED)
            pieces = [own] + [s[:, c : c + LANES] for c in range(LANES, OWNERS * blocks, LANES)]
            top = jnp.max(functools.reduce(jnp.maximum, pieces), axis=-1, keepdims=True)
            e = jnp.concatenate([jnp.exp2(p - top).astype(jnp.bfloat16) for p in pieces], axis=1)
            o = jnp.dot(e, values[...], preferred_element_type=jnp.float32)
            outs.append(o * pltpu.roll(1.0 / o, HEAD_DIM, 1))
        o = jnp.where(low_lanes(outs[0].shape), pltpu.roll(outs[0], HEAD_DIM, 1), outs[1])
        o = jnp.where(me * rows + pos >= CMP_BLOCK - 1, o, 0.0)
        g = pltpu.roll(pltpu_pad(gate[at]), LANES - 2 * rank, 1)
        oc[at] = o * gate_lanes(g, 0, o.shape)
        return carry

    def pltpu_pad(g):
        return jnp.concatenate([g, g, g, g], axis=1)

    lax.fori_loop(0, rows // part, compress, 0)

    rank_rows = rows // RANKS
    group = rank_rows // Q_BLOCK

    def mix_target(step):
        mask = RANKS - 1 - step
        return sum((rank // w + mask // w) % 2 * w for w in (4, 2, 1))

    def mix_copy(half, step):
        target = mix_target(step)
        at = pl.ds(pl.multiple_of(target * rank_rows + half * Q_BLOCK, Q_BLOCK), Q_BLOCK)
        return pltpu.make_async_remote_copy(
            src_ref=mix.at[at],
            dst_ref=heard.at[half, rank],
            send_sem=mix_send.at[half, step],
            recv_sem=mix_recv.at[half, step],
            device_id={"tp": target},
            device_id_type=MESH,
        )

    own_row = lax.broadcasted_iota(jnp.int32, (2 * Q_BLOCK, Q_BLOCK), 0)
    own_row = jnp.where(own_row >= Q_BLOCK, own_row - Q_BLOCK, own_row)
    later = lax.broadcasted_iota(jnp.int32, own_row.shape, 1) > own_row
    low_lane = lax.broadcasted_iota(jnp.int32, (1, LANES), 1) < SEL_BLOCK

    def score(j, half):
        at = pl.ds(pl.multiple_of(j * Q_BLOCK, Q_BLOCK), Q_BLOCK)
        own = j * (Q_BLOCK // SEL_BLOCK)
        parts = [held[own + b] for b in range(Q_BLOCK // SEL_BLOCK)]
        biases = []
        for a in range(FAR_PICKS):
            mark = owner_sm[a, me * q_blocks + j]
            parts.append(got[half][mark % OWNERS, j // HALVES])
            biases.append(jnp.where(mark < 64, 0.0, MASKED))
        both = jnp.concatenate(parts, axis=0)
        q = jnp.concatenate([qt[0, at], qt[1, at]], axis=0)
        return nt_dot(q, both), both, biases

    def weights(s, biases):
        pieces = [jnp.where(later, MASKED, s[:, :Q_BLOCK])]
        for a in range(0, FAR_PICKS, 2):
            c = Q_BLOCK + a * SEL_BLOCK
            pieces.append(s[:, c : c + LANES] + jnp.where(low_lane, biases[a], biases[a + 1]))
        top = jnp.max(functools.reduce(jnp.maximum, pieces), axis=-1, keepdims=True)
        return jnp.concatenate([jnp.exp2(p - top).astype(jnp.bfloat16) for p in pieces], axis=1)

    def settle(j, e, both):
        at = pl.ds(pl.multiple_of(j * Q_BLOCK, Q_BLOCK), Q_BLOCK)
        both = jnp.where(low_lanes(both.shape), jnp.ones_like(both), both)
        o = jnp.dot(e, both, preferred_element_type=jnp.float32)
        o = merge(o * pltpu.roll(1.0 / o, HEAD_DIM, 1), Q_BLOCK)
        g = pltpu.roll(pltpu_pad(gate[at]), LANES - 2 * rank, 1)
        mix[at] = (oc[at] + o * gate_lanes(g, 16, o.shape)).astype(jnp.bfloat16)

    def choose(half, i, carry):
        for step in (2 * i - 2, 2 * i - 1):
            pl.when(i > 0)(lambda step=step: mix_copy(half, step).start())
        js = [mix_target(2 * i + u) * group + half for u in range(2)]
        scored = [score(j, half) for j in js]
        es = [weights(s, biases) for s, _, biases in scored]
        for j, e, (_, both, _) in zip(js, es, scored):
            settle(j, e, both)
        return carry

    for half in range(HALVES):
        for n, (_, _, part_of) in enumerate(HOPS):
            if part_of == half:
                copy, _, _, _, gets = hop(n)
                pl.when(gets)(copy.wait_recv)
        lax.fori_loop(0, RANKS // 2, functools.partial(choose, half), 0)
        mix_copy(half, RANKS - 2).start()
        own_at = pl.ds(pl.multiple_of(rank * rank_rows + half * Q_BLOCK, Q_BLOCK), Q_BLOCK)
        heard[half, rank] = mix[own_at]

    copies[9].wait()
    for half in range(HALVES):
        for step in range(RANKS - 1):
            mix_copy(half, step).wait_recv()
        lhs = jnp.concatenate([heard[half, t] for t in range(RANKS)], axis=1)

        def finish(c, carry, half=half, lhs=lhs):
            at = pl.ds(pl.multiple_of(c * 512, 512), 512)
            y = jnp.dot(lhs, wo[:, at], preferred_element_type=jnp.float32)
            out_ref[half * Q_BLOCK : (half + 1) * Q_BLOCK, at] = y.astype(jnp.bfloat16)
            return carry

        lax.fori_loop(0, width // 512, finish, 0)

    for n in range(len(MOVES)):
        copy, _, sends, _ = sum_copy(n, me)
        pl.when(sends)(copy.wait_send)
    for n in range(len(HOPS)):
        copy, _, _, sends, _ = hop(n)
        pl.when(sends)(copy.wait_send)
    for n in range(4):
        for c in range(tiles):
            copy, sends = span_copy(n, c)
            pl.when(sends)(copy.wait_send)
    for half in range(HALVES):
        for step in range(RANKS - 1):
            mix_copy(half, step).wait_send()


def rope_tables(length):
    half = HEAD_DIM // 2
    inverse = ROPE_BASE ** (-(np.arange(half, dtype=np.float32)) / np.float32(half))
    inverse = np.tile(inverse.astype(np.float32).astype(np.float64), LANES // half)

    def table(positions):
        angle = positions.astype(np.float64)[:, None] * inverse[None, :]
        return np.cos(angle), np.sin(angle)

    low = np.concatenate(table(np.arange(SEL_BLOCK)), axis=0).astype(np.float32)
    high = np.concatenate(table(np.arange(length // SEL_BLOCK) * SEL_BLOCK), axis=1).astype(np.float32)
    return jnp.asarray(low), jnp.asarray(high)


def per_device(
    tokens,
    norm_gain,
    query_weight,
    cmp_key_weight,
    cmp_value_weight,
    sel_key_weight,
    sel_value_weight,
    branch_weight,
    key_embed,
    key_inner,
    key_outer,
    value_embed,
    value_inner,
    value_outer,
    out_weight,
    chosen,
):
    rows, width = tokens.shape
    f32, bf16 = jnp.float32, jnp.bfloat16
    low, high = rope_tables(rows * OWNERS)
    span = rows // SEL_BLOCK
    q_blocks = rows // Q_BLOCK
    blocks = rows // CMP_BLOCK
    rank_rows = rows // RANKS
    picks = chosen.shape[1]
    operands = (
        chosen[0].T,
        norm_gain,
        key_embed[0],
        key_outer[0],
        value_embed[0],
        value_outer[0],
        low,
        high,
        tokens,
        query_weight,
        sel_key_weight.T,
        sel_value_weight.T,
        cmp_key_weight.T,
        cmp_value_weight.T,
        branch_weight.transpose(0, 2, 1).reshape(32, width),
        key_inner[0].T,
        value_inner[0].T,
        out_weight,
    )
    vmem = pl.BlockSpec(memory_space=pltpu.VMEM)
    hbm = pl.BlockSpec(memory_space=pl.ANY)
    dma = pltpu.SemaphoreType.DMA
    moves = len(MOVES)
    return pl.pallas_call(
        layer_kernel,
        in_specs=[vmem] * 7 + [hbm] * 11,
        out_specs=vmem,
        out_shape=pltpu.VMEM((rank_rows, width), bf16),
        scratch_shapes=[
            pltpu.VMEM((span, 2 * LANES), f32),
            pltpu.VMEM((rows, width), bf16),
            pltpu.VMEM((width, LANES), bf16),
            pltpu.VMEM((288, width), bf16),
            pltpu.VMEM((416, width), bf16),
            pltpu.VMEM((HEAD_DIM, width), bf16),
            pltpu.VMEM((HEAD_DIM, width), bf16),
            pltpu.VMEM(out_weight.shape, bf16),
            pltpu.VMEM((span, SEL_BLOCK, LANES), bf16),
            pltpu.VMEM((span, SEL_BLOCK, LANES), bf16),
            pltpu.VMEM((span, SEL_BLOCK, LANES), bf16),
            pltpu.VMEM((len(HOPS), q_blocks // HALVES, SEL_BLOCK, LANES), bf16),
            pltpu.VMEM((OWNERS, q_blocks // HALVES, SEL_BLOCK, LANES), bf16),
            pltpu.VMEM((OWNERS, q_blocks // HALVES, SEL_BLOCK, LANES), bf16),
            pltpu.VMEM((2, rows, LANES), bf16),
            pltpu.VMEM((2, rows, LANES), bf16),
            pltpu.VMEM((rows, LANES), f32),
            pltpu.VMEM((rows, 32), f32),
            pltpu.VMEM((rows, LANES), f32),
            pltpu.VMEM((OWNERS, blocks, LANES), bf16),
            pltpu.VMEM((OWNERS * blocks, LANES), bf16),
            pltpu.VMEM((OWNERS * blocks, LANES), bf16),
            pltpu.VMEM((rows, LANES), f32),
            pltpu.VMEM((rows, LANES), bf16),
            pltpu.VMEM((HALVES, RANKS, Q_BLOCK, LANES), bf16),
            pltpu.VMEM((2, FAR_PICKS, picks), jnp.int32),
            pltpu.SMEM((FAR_PICKS, picks), jnp.int32),
            pltpu.SMEM((FAR_PICKS, picks), jnp.int32),
            dma((rows // 512,)),
            dma((12,)),
            dma((4, 4)),
            dma((2, 4)),
            dma((len(HOPS),)),
            dma((len(HOPS),)),
            dma((moves,)),
            dma((moves,)),
            dma((HALVES, RANKS)),
            dma((HALVES, RANKS)),
        ],
        compiler_params=pltpu.CompilerParams(
            collective_id=0, has_side_effects=True, vmem_limit_bytes=60 * 1024 * 1024
        ),
        cost_estimate=pl.CostEstimate(flops=int(4e10), bytes_accessed=int(2e7), transcendentals=0),
        name="layer",
    )(*operands)


def solution(mesh):
    placed = (
        P("kv", None),
        P(),
        P(None, "tp"),
        P(None, "tp"),
        P(None, "tp"),
        P(None, "tp"),
        P(None, "tp"),
        P(),
        P("tp", None, None),
        P("tp", None, None),
        P("tp", None, None),
        P("tp", None, None),
        P("tp", None, None),
        P("tp", None, None),
        P(),
        P("tp", None, None),
    )
    return jax.shard_map(
        per_device, mesh=mesh, in_specs=placed, out_specs=P(("kv", "tp"), None), check_vma=False
    )
```

```python
import functools
import math

import jax
import jax.numpy as jnp
import numpy as np
from jax import lax
from jax.experimental import pallas as pl
from jax.experimental.pallas import tpu as pltpu
from jax.sharding import PartitionSpec as P

HEAD_DIM = 64
CMP_BLOCK = 32
SEL_BLOCK = 64
Q_BLOCK = 128
FAR_PICKS = 8
LANES = 2 * HEAD_DIM
PLANES = 4
ACROSS = 4
OWNERS = PLANES * ACROSS
RANKS = 8
MESH = pl.DeviceIdType.MESH

ROPE_BASE = 10000.0
norm_eps = 1e-06
MASKED = -1e30

MOVES = [(dz, dx) for dx in (2, 1, 3, 0) for dz in (2, 1, 3, 0) if (dz, dx) != (0, 0)]
OWN, NEAR, FAR, SKIP = range(4)
HALVES = 2
HOPS = [(OWN, dx, half) for half in range(HALVES) for dx in (2, 1, 3)]
for half in range(HALVES):
    HOPS += [(SKIP, dx, half) for dx in (0, 1, 3, 2)]
    HOPS += [(kind, dx, half) for kind in (NEAR, FAR) for dx in (2, 1, 3)]


def nt_dot(a, b):
    return lax.dot_general(a, b, (((1,), (1,)), ((), ())), preferred_element_type=jnp.float32)


def low_lanes(shape):
    return lax.broadcasted_iota(jnp.int32, shape, 1) < HEAD_DIM


def gate_lanes(gate, first, shape):
    return jnp.where(low_lanes(shape), gate[:, first : first + 1], gate[:, first + 1 : first + 2])


def merge(out, rows):
    low = low_lanes((rows, LANES))
    return jnp.where(low, pltpu.roll(out[:rows], HEAD_DIM, 1), out[rows:])


def layer_kernel(
    chosen_ref,
    gain_ref,
    ke_ref,
    ko_ref,
    ve_ref,
    vo_ref,
    lo_ref,
    hi_hbm,
    tok_hbm,
    wq_hbm,
    wsk_hbm,
    wsv_hbm,
    wck_hbm,
    wcv_hbm,
    wg_hbm,
    ki_hbm,
    vi_hbm,
    wo_hbm,
    out_ref,
    hi,
    tok,
    wq,
    raw,
    wt,
    ki,
    vi,
    wo,
    held,
    near,
    far,
    stage,
    got_even,
    got_odd,
    qp,
    qt,
    ckv,
    gate,
    scales,
    sums,
    keys,
    values,
    oc,
    mix,
    heard,
    pick_vm,
    pick_sm,
    owner_sm,
    tok_sem,
    local_sem,
    span_send,
    span_recv,
    send_sem,
    recv_sem,
    sum_send,
    sum_recv,
    mix_send,
    mix_recv,
):
    me, rank = lax.axis_index("kv"), lax.axis_index("tp")
    z, x = me // ACROSS, me % ACROSS
    rows, width = tok.shape
    tile = 512
    tiles = rows // tile
    q_blocks = rows // Q_BLOCK
    span = rows // SEL_BLOCK
    blocks = rows // CMP_BLOCK
    got = (got_even, got_odd)
    scale = HEAD_DIM ** (-0.5) * math.log2(math.e)

    sums[...] = jnp.zeros_like(sums)
    barrier = pltpu.get_barrier_semaphore()
    for d in range(1, OWNERS):
        pl.semaphore_signal(barrier, inc=1, device_id={"kv": (me + d) % OWNERS}, device_id_type=MESH)
    for d in range(1, RANKS):
        pl.semaphore_signal(barrier, inc=1, device_id={"tp": (rank + d) % RANKS}, device_id_type=MESH)

    loads = [
        (wq_hbm, wq),
        (wsk_hbm, raw.at[pl.ds(0, 64)]),
        (wsv_hbm, raw.at[pl.ds(64, 64)]),
        (wck_hbm, raw.at[pl.ds(128, 64)]),
        (wcv_hbm, raw.at[pl.ds(192, 64)]),
        (wg_hbm, raw.at[pl.ds(256, 32)]),
        (hi_hbm.at[pl.ds(pl.multiple_of(me * span, span), span)], hi),
        (ki_hbm, ki),
        (vi_hbm, vi),
        (wo_hbm, wo),
    ]
    copies = [pltpu.make_async_copy(a, b, local_sem.at[n]) for n, (a, b) in enumerate(loads)]
    tok_copies = [
        pltpu.make_async_copy(tok_hbm.at[pl.ds(n * tile, tile)], tok.at[pl.ds(n * tile, tile)], tok_sem.at[n])
        for n in range(tiles)
    ]
    for copy in copies[:7]:
        copy.start()
    for copy in tok_copies:
        copy.start()
    for copy in copies[7:]:
        copy.start()

    chosen = chosen_ref[...]
    near_owner, far_owner = jnp.where(z == 0, me + ACROSS, me - ACROSS), x
    line = lax.broadcasted_iota(jnp.int32, chosen.shape, 0)
    index = jnp.zeros(chosen.shape, jnp.int32)
    for kind, owner in ((OWN, me), (NEAR, near_owner), (FAR, far_owner)):
        inside = jnp.where(chosen // span == owner, chosen % span, 0)
        index = jnp.where(line == kind, jnp.sum(inside, axis=0, keepdims=True), index)
    pick_vm[0] = index
    at_block = lax.broadcasted_iota(jnp.int32, chosen.shape, 1) * (Q_BLOCK // SEL_BLOCK)
    pick_vm[1] = jnp.where(chosen < at_block, chosen // span, 64 + me)
    to_smem = pltpu.make_async_copy(pick_vm.at[0], pick_sm, local_sem.at[len(loads)])
    owner_smem = pltpu.make_async_copy(pick_vm.at[1], owner_sm, local_sem.at[len(loads) + 1])
    to_smem.start()
    owner_smem.start()

    for copy in copies[:7]:
        copy.wait()

    gain = gain_ref[...].astype(jnp.float32).reshape(1, width)
    eye = (
        lax.broadcasted_iota(jnp.int32, (LANES, LANES), 0)
        == lax.broadcasted_iota(jnp.int32, (LANES, LANES), 1)
    ).astype(jnp.bfloat16)

    def weigh(source, first, count, target):
        def one(i, carry):
            r = pl.ds(pl.multiple_of(first + i * 16, 16), 16)
            t = pl.ds(pl.multiple_of(target + i * 16, 16), 16)
            wt[t] = (source[r].astype(jnp.float32) * gain).astype(jnp.bfloat16)
            return carry

        lax.fori_loop(0, count // 16, one, 0)

    weigh(raw, 0, 128, 0)
    for c in range(width // 256):
        cut = slice(c * 256, (c + 1) * 256)
        turned = nt_dot(eye, wq[cut])
        wt[128:256, cut] = (turned * gain[:, cut]).astype(jnp.bfloat16)

    first_half = lax.broadcasted_iota(jnp.int32, (1, LANES), 1) % HEAD_DIM < HEAD_DIM // 2
    flag = (lax.broadcasted_iota(jnp.int32, (1, LANES), 1) == HEAD_DIM).astype(jnp.float32)
    quarter = HEAD_DIM // 2

    def turn(v, cosine, sine):
        swapped = jnp.where(first_half, pltpu.roll(v, LANES - quarter, 1), pltpu.roll(v, quarter, 1))
        return v * cosine + swapped * sine

    def project(i):
        at = pl.ds(i * tile, tile)
        v = tok[at]
        y = nt_dot(v, wt[0:256])
        w = v.astype(jnp.float32)
        inv = lax.rsqrt(jnp.mean(w * w, axis=-1, keepdims=True) + norm_eps)
        scales[at] = jnp.broadcast_to(inv, (tile, LANES))
        y = y * inv
        cos_lo, sin_lo = lo_ref[0:64], lo_ref[64:128]
        for g in range(tile // SEL_BLOCK):
            b = i * (tile // SEL_BLOCK) + g
            cut = slice(g * SEL_BLOCK, (g + 1) * SEL_BLOCK)
            cos_hi, sin_hi = hi[pl.ds(b, 1), 0:LANES], hi[pl.ds(b, 1), LANES : 2 * LANES]
            cosine = cos_hi * cos_lo - sin_hi * sin_lo
            sine = sin_hi * cos_lo + cos_hi * sin_lo
            sine = jnp.where(first_half, -sine, sine)
            part = y[cut, 0:LANES]
            low = low_lanes(part.shape)
            held[b] = jnp.where(low, turn(part, cosine, sine), part).astype(jnp.bfloat16)
            part = y[cut, LANES : 2 * LANES] * scale
            to = pl.ds(b * SEL_BLOCK, SEL_BLOCK)
            for ref, q, rest in ((qp, part, flag), (qt, turn(part, cosine, sine), 0.0)):
                ref[0, to] = jnp.where(low, q, rest).astype(jnp.bfloat16)
                ref[1, to] = jnp.where(low, pltpu.roll(q, HEAD_DIM, 1), rest).astype(jnp.bfloat16)

    def route(dz, dx):
        there = ((z + dz) % PLANES) * ACROSS + (x + dx) % ACROSS
        here = ((z - dz) % PLANES) * ACROSS + (x - dx) % ACROSS
        if dz == 0:
            return there, x + dx < ACROSS, here, x >= dx
        return there, z + dz < PLANES, here, z >= dz

    def span_copy(n, c):
        step, sends, source, target = (
            (1, z < 3, held, near),
            (3, z == 1, held, near),
            (3, z == 0, held, far),
            (3, z == 3, far, far),
        )[n]
        at = pl.ds(c * (span // tiles), span // tiles)
        return (
            pltpu.make_async_remote_copy(
                src_ref=source.at[at],
                dst_ref=target.at[at],
                send_sem=span_send.at[n, c],
                recv_sem=span_recv.at[n // 2, c],
                device_id={"kv": lax.rem(me + step * ACROSS, OWNERS)},
                device_id_type=MESH,
            ),
            sends,
        )

    for i in range(tiles):
        tok_copies[i].wait()
        project(i)
        if i == 0:
            pl.semaphore_wait(barrier, OWNERS + RANKS - 2)
        for n in range(3):
            copy, sends = span_copy(n, i)
            pl.when(sends)(copy.start)

    to_smem.wait()
    owner_smem.wait()

    def hop(n):
        kind, dx, half = HOPS[n]
        column = lax.rem(x + dx, ACROSS)
        back = lax.rem(x + ACROSS - dx, ACROSS)
        if kind == OWN:
            owner, source, sends, gets = me, held, x + dx < ACROSS, x >= dx
        elif kind == NEAR:
            owner, source, sends, gets = near_owner, near, z >= 1, z >= 1
        elif kind == FAR:
            owner, source, sends, gets = far_owner, far, z >= 2, z >= 2
        else:
            owner, source, sends, gets = near_owner, near, z == (2 if dx == 0 else 0), z == 3
        there = (3 if kind == SKIP else z) * ACROSS + column
        copy = pltpu.make_async_remote_copy(
            src_ref=stage.at[n],
            dst_ref=got[half].at[owner],
            send_sem=send_sem.at[n],
            recv_sem=recv_sem.at[n],
            device_id={"kv": there},
            device_id_type=MESH,
        )
        return copy, there, source, sends, gets

    def gather(source, kind, target, first):
        def one(p, carry):
            target[p] = source[pick_sm[kind, first + HALVES * p]]
            return carry

        lax.fori_loop(0, q_blocks // HALVES, one, 0)

    def gather_own(source, kind, owner):
        for half in range(HALVES):
            gather(source, kind, got[half].at[owner], me * q_blocks + half)

    def send_hops(which, part):
        for n, (kind, dx, half) in enumerate(HOPS):
            if kind == which and half == part:
                copy, there, source, sends, _ = hop(n)

                def go(n=n, kind=kind, copy=copy, there=there, source=source):
                    first = there * q_blocks + part
                    gather(source, NEAR if kind == SKIP else kind, stage.at[n], first)
                    copy.start()

                pl.when(sends)(go)

    for half in range(HALVES):
        send_hops(OWN, half)

    weigh(raw, 128, 160, 256)

    def project_more(i):
        at = pl.ds(i * tile, tile)
        y = nt_dot(tok[at], wt[256:416])
        inv = scales[at]
        ckv[at] = (y[:, 0:LANES] * inv).astype(jnp.bfloat16).astype(jnp.float32)
        gate[at] = jax.nn.sigmoid(y[:, LANES : LANES + 32] * inv[:, 0:32])

    def hand_back(c):
        span_copy(2, c)[0].wait_recv()
        span_copy(3, c)[0].start()

    for c in range(tiles):
        project_more(c)
        pl.when(z == 3)(functools.partial(hand_back, c))
    for copy in copies[7:9]:
        copy.wait()

    low = low_lanes((blocks, LANES))

    def summarize(is_value, e_ref, i_ref, o_ref):
        parts = []
        embed = e_ref[...].astype(jnp.float32)
        for c in range(0, CMP_BLOCK, 2):
            a = ckv[pl.ds(c, blocks, stride=CMP_BLOCK), :]
            b = ckv[pl.ds(c + 1, blocks, stride=CMP_BLOCK), :]
            if is_value:
                pair = jnp.where(low, pltpu.roll(a, HEAD_DIM, 1), b)
            else:
                pair = jnp.where(low, a, pltpu.roll(b, HEAD_DIM, 1))
            e = jnp.concatenate([embed[c : c + 1], embed[c + 1 : c + 2]], axis=1)
            parts.append((pair + e).astype(jnp.bfloat16))
        flat = jnp.concatenate(parts, axis=1)
        hidden = jax.nn.gelu(nt_dot(flat, i_ref[...])).astype(jnp.bfloat16)
        return jnp.dot(hidden, o_ref[...], preferred_element_type=jnp.float32)

    sk = summarize(False, ke_ref, ki, ko_ref)
    sv = summarize(True, ve_ref, vi, vo_ref)
    sums[me] = jnp.concatenate([sk, sv], axis=1).astype(jnp.bfloat16)

    def sum_copy(n, owner):
        there, sends, here, gets = route(*MOVES[n])
        copy = pltpu.make_async_remote_copy(
            src_ref=sums.at[owner],
            dst_ref=sums.at[owner],
            send_sem=sum_send.at[n],
            recv_sem=sum_recv.at[n],
            device_id={"kv": there},
            device_id_type=MESH,
        )
        return copy, here, sends, gets

    for n in range(len(MOVES)):
        copy, _, sends, _ = sum_copy(n, me)
        pl.when(sends)(copy.start)
    gather_own(held, OWN, me)
    for c in range(tiles):
        span_copy(0, c)[0].wait_recv()
    for half in range(HALVES):
        send_hops(SKIP, half)
        pl.when(z == 3)(functools.partial(send_hops, FAR, half))
        send_hops(NEAR, half)
        if half == 0:
            for c in range(tiles):
                pl.when(z == 2)(span_copy(2, c)[0].wait_recv)
        pl.when(z == 2)(functools.partial(send_hops, FAR, half))
    pl.when(z >= 1)(lambda: gather_own(near, NEAR, near_owner))
    pl.when(z >= 2)(lambda: gather_own(far, FAR, far_owner))
    for n in range(len(MOVES)):
        _, here, _, gets = sum_copy(n, me)
        copy, _, _, _ = sum_copy(n, here)
        pl.when(gets)(copy.wait_recv)

    lane = lax.broadcasted_iota(jnp.int32, (blocks, LANES), 1)
    for d in range(OWNERS):
        owner = lax.rem(me + d, OWNERS)
        both = sums[owner]
        bar = jnp.where(owner > me, MASKED, 0.0).astype(jnp.bfloat16)
        rows_at = slice(d * blocks, (d + 1) * blocks)
        keys[rows_at] = jnp.where(lane == HEAD_DIM, bar, both)
        values[rows_at] = jnp.where(lane < HEAD_DIM, jnp.ones_like(both), both)

    part = 256

    def compress(i, carry):
        at = pl.ds(pl.multiple_of(i * part, part), part)
        pos = i * part + lax.broadcasted_iota(jnp.int32, (part, 1), 0)
        lane = lax.broadcasted_iota(jnp.int32, (1, LANES), 1)
        scored = [nt_dot(qp[h, at], keys[...]) for h in range(2)]
        outs = []
        for s in scored:
            own = jnp.where((lane >= blocks) | ((lane + 1) * CMP_BLOCK - 1 <= pos), s[:, :LANES], MASKED)
            pieces = [own] + [s[:, c : c + LANES] for c in range(LANES, OWNERS * blocks, LANES)]
            top = jnp.max(functools.reduce(jnp.maximum, pieces), axis=-1, keepdims=True)
            e = jnp.concatenate([jnp.exp2(p - top).astype(jnp.bfloat16) for p in pieces], axis=1)
            o = jnp.dot(e, values[...], preferred_element_type=jnp.float32)
            outs.append(o * pltpu.roll(1.0 / o, HEAD_DIM, 1))
        o = jnp.where(low_lanes(outs[0].shape), pltpu.roll(outs[0], HEAD_DIM, 1), outs[1])
        o = jnp.where(me * rows + pos >= CMP_BLOCK - 1, o, 0.0)
        g = pltpu.roll(pltpu_pad(gate[at]), LANES - 2 * rank, 1)
        oc[at] = o * gate_lanes(g, 0, o.shape)
        return carry

    def pltpu_pad(g):
        return jnp.concatenate([g, g, g, g], axis=1)

    lax.fori_loop(0, rows // part, compress, 0)

    rank_rows = rows // RANKS
    group = rank_rows // Q_BLOCK

    def mix_target(step):
        mask = RANKS - 1 - step
        return sum((rank // w + mask // w) % 2 * w for w in (4, 2, 1))

    def mix_copy(half, step):
        target = mix_target(step)
        at = pl.ds(pl.multiple_of(target * rank_rows + half * Q_BLOCK, Q_BLOCK), Q_BLOCK)
        return pltpu.make_async_remote_copy(
            src_ref=mix.at[at],
            dst_ref=heard.at[half, rank],
            send_sem=mix_send.at[half, step],
            recv_sem=mix_recv.at[half, step],
            device_id={"tp": target},
            device_id_type=MESH,
        )

    own_row = lax.broadcasted_iota(jnp.int32, (2 * Q_BLOCK, Q_BLOCK), 0)
    own_row = jnp.where(own_row >= Q_BLOCK, own_row - Q_BLOCK, own_row)
    later = lax.broadcasted_iota(jnp.int32, own_row.shape, 1) > own_row
    low_lane = lax.broadcasted_iota(jnp.int32, (1, LANES), 1) < SEL_BLOCK

    def score(j, half):
        at = pl.ds(pl.multiple_of(j * Q_BLOCK, Q_BLOCK), Q_BLOCK)
        own = j * (Q_BLOCK // SEL_BLOCK)
        parts = [held[own + b] for b in range(Q_BLOCK // SEL_BLOCK)]
        biases = []
        for a in range(FAR_PICKS):
            mark = owner_sm[a, me * q_blocks + j]
            parts.append(got[half][mark % OWNERS, j // HALVES])
            biases.append(jnp.where(mark < 64, 0.0, MASKED))
        both = jnp.concatenate(parts, axis=0)
        q = jnp.concatenate([qt[0, at], qt[1, at]], axis=0)
        return nt_dot(q, both), both, biases

    def weights(s, biases):
        pieces = [jnp.where(later, MASKED, s[:, :Q_BLOCK])]
        for a in range(0, FAR_PICKS, 2):
            c = Q_BLOCK + a * SEL_BLOCK
            pieces.append(s[:, c : c + LANES] + jnp.where(low_lane, biases[a], biases[a + 1]))
        top = jnp.max(functools.reduce(jnp.maximum, pieces), axis=-1, keepdims=True)
        return jnp.concatenate([jnp.exp2(p - top).astype(jnp.bfloat16) for p in pieces], axis=1)

    def settle(j, e, both):
        at = pl.ds(pl.multiple_of(j * Q_BLOCK, Q_BLOCK), Q_BLOCK)
        both = jnp.where(low_lanes(both.shape), jnp.ones_like(both), both)
        o = jnp.dot(e, both, preferred_element_type=jnp.float32)
        o = merge(o * pltpu.roll(1.0 / o, HEAD_DIM, 1), Q_BLOCK)
        g = pltpu.roll(pltpu_pad(gate[at]), LANES - 2 * rank, 1)
        mix[at] = (oc[at] + o * gate_lanes(g, 16, o.shape)).astype(jnp.bfloat16)

    def choose(half, i, carry):
        for step in (2 * i - 2, 2 * i - 1):
            pl.when(i > 0)(lambda step=step: mix_copy(half, step).start())
        js = [mix_target(2 * i + u) * group + half for u in range(2)]
        scored = [score(j, half) for j in js]
        es = [weights(s, biases) for s, _, biases in scored]
        for j, e, (_, both, _) in zip(js, es, scored):
            settle(j, e, both)
        return carry

    for half in range(HALVES):
        for n, (_, _, part_of) in enumerate(HOPS):
            if part_of == half:
                copy, _, _, _, gets = hop(n)
                pl.when(gets)(copy.wait_recv)
        lax.fori_loop(0, RANKS // 2, functools.partial(choose, half), 0)
        mix_copy(half, RANKS - 2).start()
        own_at = pl.ds(pl.multiple_of(rank * rank_rows + half * Q_BLOCK, Q_BLOCK), Q_BLOCK)
        heard[half, rank] = mix[own_at]

    copies[9].wait()
    for half in range(HALVES):
        for step in range(RANKS - 1):
            mix_copy(half, step).wait_recv()
        lhs = jnp.concatenate([heard[half, t] for t in range(RANKS)], axis=1)

        def finish(c, carry, half=half, lhs=lhs):
            at = pl.ds(pl.multiple_of(c * 512, 512), 512)
            y = jnp.dot(lhs, wo[:, at], preferred_element_type=jnp.float32)
            out_ref[half * Q_BLOCK : (half + 1) * Q_BLOCK, at] = y.astype(jnp.bfloat16)
            return carry

        lax.fori_loop(0, width // 512, finish, 0)

    for n in range(len(MOVES)):
        copy, _, sends, _ = sum_copy(n, me)
        pl.when(sends)(copy.wait_send)
    for n in range(len(HOPS)):
        copy, _, _, sends, _ = hop(n)
        pl.when(sends)(copy.wait_send)
    for n in range(4):
        for c in range(tiles):
            copy, sends = span_copy(n, c)
            pl.when(sends)(copy.wait_send)
    for half in range(HALVES):
        for step in range(RANKS - 1):
            mix_copy(half, step).wait_send()


def rope_tables(length):
    half = HEAD_DIM // 2
    inverse = ROPE_BASE ** (-(np.arange(half, dtype=np.float32)) / np.float32(half))
    inverse = np.tile(inverse.astype(np.float32).astype(np.float64), LANES // half)

    def table(positions):
        angle = positions.astype(np.float64)[:, None] * inverse[None, :]
        return np.cos(angle), np.sin(angle)

    low = np.concatenate(table(np.arange(SEL_BLOCK)), axis=0).astype(np.float32)
    high = np.concatenate(table(np.arange(length // SEL_BLOCK) * SEL_BLOCK), axis=1).astype(np.float32)
    return jnp.asarray(low), jnp.asarray(high)


def per_device(
    tokens,
    norm_gain,
    query_weight,
    cmp_key_weight,
    cmp_value_weight,
    sel_key_weight,
    sel_value_weight,
    branch_weight,
    key_embed,
    key_inner,
    key_outer,
    value_embed,
    value_inner,
    value_outer,
    out_weight,
    chosen,
):
    rows, width = tokens.shape
    f32, bf16 = jnp.float32, jnp.bfloat16
    low, high = rope_tables(rows * OWNERS)
    span = rows // SEL_BLOCK
    q_blocks = rows // Q_BLOCK
    blocks = rows // CMP_BLOCK
    rank_rows = rows // RANKS
    picks = chosen.shape[1]
    operands = (
        chosen[0].T,
        norm_gain,
        key_embed[0],
        key_outer[0],
        value_embed[0],
        value_outer[0],
        low,
        high,
        tokens,
        query_weight,
        sel_key_weight.T,
        sel_value_weight.T,
        cmp_key_weight.T,
        cmp_value_weight.T,
        branch_weight.transpose(0, 2, 1).reshape(32, width),
        key_inner[0].T,
        value_inner[0].T,
        out_weight,
    )
    vmem = pl.BlockSpec(memory_space=pltpu.VMEM)
    hbm = pl.BlockSpec(memory_space=pl.ANY)
    dma = pltpu.SemaphoreType.DMA
    moves = len(MOVES)
    return pl.pallas_call(
        layer_kernel,
        in_specs=[vmem] * 7 + [hbm] * 11,
        out_specs=vmem,
        out_shape=pltpu.VMEM((rank_rows, width), bf16),
        scratch_shapes=[
            pltpu.VMEM((span, 2 * LANES), f32),
            pltpu.VMEM((rows, width), bf16),
            pltpu.VMEM((width, LANES), bf16),
            pltpu.VMEM((288, width), bf16),
            pltpu.VMEM((416, width), bf16),
            pltpu.VMEM((HEAD_DIM, width), bf16),
            pltpu.VMEM((HEAD_DIM, width), bf16),
            pltpu.VMEM(out_weight.shape, bf16),
            pltpu.VMEM((span, SEL_BLOCK, LANES), bf16),
            pltpu.VMEM((span, SEL_BLOCK, LANES), bf16),
            pltpu.VMEM((span, SEL_BLOCK, LANES), bf16),
            pltpu.VMEM((len(HOPS), q_blocks // HALVES, SEL_BLOCK, LANES), bf16),
            pltpu.VMEM((OWNERS, q_blocks // HALVES, SEL_BLOCK, LANES), bf16),
            pltpu.VMEM((OWNERS, q_blocks // HALVES, SEL_BLOCK, LANES), bf16),
            pltpu.VMEM((2, rows, LANES), bf16),
            pltpu.VMEM((2, rows, LANES), bf16),
            pltpu.VMEM((rows, LANES), f32),
            pltpu.VMEM((rows, 32), f32),
            pltpu.VMEM((rows, LANES), f32),
            pltpu.VMEM((OWNERS, blocks, LANES), bf16),
            pltpu.VMEM((OWNERS * blocks, LANES), bf16),
            pltpu.VMEM((OWNERS * blocks, LANES), bf16),
            pltpu.VMEM((rows, LANES), f32),
            pltpu.VMEM((rows, LANES), bf16),
            pltpu.VMEM((HALVES, RANKS, Q_BLOCK, LANES), bf16),
            pltpu.VMEM((2, FAR_PICKS, picks), jnp.int32),
            pltpu.SMEM((FAR_PICKS, picks), jnp.int32),
            pltpu.SMEM((FAR_PICKS, picks), jnp.int32),
            dma((rows // 512,)),
            dma((12,)),
            dma((4, 4)),
            dma((2, 4)),
            dma((len(HOPS),)),
            dma((len(HOPS),)),
            dma((moves,)),
            dma((moves,)),
            dma((HALVES, RANKS)),
            dma((HALVES, RANKS)),
        ],
        compiler_params=pltpu.CompilerParams(
            collective_id=0, has_side_effects=True, vmem_limit_bytes=60 * 1024 * 1024
        ),
        cost_estimate=pl.CostEstimate(flops=int(4e10), bytes_accessed=int(2e7), transcendentals=0),
        name="layer",
    )(*operands)


def solution(mesh):
    placed = (
        P("kv", None),
        P(),
        P(None, "tp"),
        P(None, "tp"),
        P(None, "tp"),
        P(None, "tp"),
        P(None, "tp"),
        P(),
        P("tp", None, None),
        P("tp", None, None),
        P("tp", None, None),
        P("tp", None, None),
        P("tp", None, None),
        P("tp", None, None),
        P(),
        P("tp", None, None),
    )
    return jax.shard_map(
        per_device, mesh=mesh, in_specs=placed, out_specs=P(("kv", "tp"), None), check_vma=False
    )
```
